32 devices in a mesh: ep: 4 (over y, x), tp: 8 (over z, core).
Axes of the slice: x: 2, y: 2, z: 4, core: 2. Of those that a mesh axis runs over, the one named last changes fastest.
Arguments:
- mix_query: bfloat16 [2048, 2048], P('ep', 'tp'), may hold values from -60 to 60
- mix_key: bfloat16 [2048, 2048], P('ep', 'tp'), may hold values from -60 to 60
- mix_value: bfloat16 [2048, 2048], P('ep', 'tp'), may hold values from -6 to 6
- head_lambda: float32 [16], P('tp'), may hold values from 0.3 to 0.8
- head_gain: float32 [128], replicated, may hold values from 0.1 to 1.9
- out_weight: bfloat16 [2048, 2048], P('tp'), may hold values from -0.125 to 0.125
- moe_input: bfloat16 [2048, 2048], P(('ep', 'tp')), may hold values from -6 to 6
- moe_gain: float32 [2048], replicated, may hold values from 0.1 to 1.9
- expert_ids: int32 [2048, 2], P(('ep', 'tp')), may hold values from 0 to 3, all different within a row; in each aligned block of 64 rows (0 to 63, 64 to 127, ...) at most 48 rows name the same one
- route_weight: float32 [2048, 2], P(('ep', 'tp')), may hold values from 0.2 to 1
- gate_weight: bfloat16 [4, 2048, 4096], P('ep', None, 'tp'), may hold values from -0.125 to 0.125
- up_weight: bfloat16 [4, 2048, 4096], P('ep', None, 'tp'), may hold values from -0.125 to 0.125
- down_weight: bfloat16 [4, 4096, 2048], P('ep', 'tp'), may hold values from -0.09375 to 0.09375
Outputs:
- mix_output: bfloat16 [2048, 2048], P(('ep', 'tp'))
- moe_output: bfloat16 [2048, 2048], P(('ep', 'tp'))
The draws below stay inside these ranges and needn't reach their ends.
Inputs may be any that keep to these rules, and one draw needn't show every extreme that they name: `expert_ids`: in each aligned block of 64 rows (the rows of one device) no expert is named by more than 48 rows; a row names 2 different experts.
All inputs are finite; a program needn't handle non-finite values.
Results may differ from the reference program's by a relative error of at most 0.02.
The reference program's roundings to bfloat16 on the way count: a program that leaves them out, or rounds other values in their place, can miss the bound.
Values may be sent and summed in bfloat16 or wider, within the bound.
A program may use at most 128 MiB of HBM per device.

```python
import math
import jax
import jax.numpy as jnp
import numpy as np
from jax import lax

D = 2048
HEADS = 16
HD = 64
FF = 4096
TOP = 2
ROWS_B = 64
VD = 128
HEADS_DEV = 2
FF_DEV = 512
EXPERTS = 4
CAP = 48
SEQ = 2048
TOKENS_B = 2048
N_TP = 8


def draw_query_side(key, stream):
    columns = HEADS * 2 * HD
    return jnp.clip(1.3 * jax.random.normal(jax.random.fold_in(key, stream), (SEQ, columns), jnp.float32), -8.0, 8.0)


def draw_mix_query(key, part):
    return draw_query_side(key, 11).astype(jnp.bfloat16)


def draw_mix_key(key, part):
    return draw_query_side(key, 13).astype(jnp.bfloat16)


def level_of(stream_key, extent, cuts, least, largest):
    factor_of, own = 1.0, jax.random.fold_in(stream_key, 6)
    for axis_at, parts in cuts:
        draws = jnp.exp(jax.random.uniform(jax.random.fold_in(own, axis_at), (parts,), jnp.float32, least / len(cuts), largest / len(cuts)))
        factor_of = factor_of * jnp.repeat(draws, extent[axis_at] // parts).reshape([-1 if axis == axis_at else 1 for axis in range(len(extent))])
    return factor_of


def assign_block(key, own, number, rows, number_of, top, most, lean):
    order = jax.random.permutation(key, number_of)
    packed, common = shares(number_of, rows * top, most, lean, True), shares(number_of, rows * top, most, lean, False)
    places = jnp.arange(number_of)

    def named(sizes, rotation):
        used = int((sizes > 0).sum())
        fixed = max(1, used // 4)
        passed = fixed + (places - fixed + rotation * (used - fixed)) % max(1, number_of - fixed)
        return jnp.zeros((number_of,), jnp.int32).at[order[jnp.where(places < fixed, places, passed)]].set(jnp.asarray(sizes, jnp.int32))

    sizes = jnp.where(number % 4 == 0, named(packed, number // 4), named(common, number - number // 4 - 1))
    mixed = jax.random.permutation(jax.random.fold_in(own, 3), number_of)
    source_of, receiver = mixed[0:number_of // 2 * 2:2], mixed[1:number_of // 2 * 2:2]
    room = jnp.minimum(sizes[source_of] - 1, most - sizes[receiver]) // 2
    room = jnp.where((source_of == order[0]) | (receiver == order[0]) | (sizes[receiver] == 0), 0, jnp.maximum(room, 0))
    passed = jax.random.randint(jax.random.fold_in(own, 4), (number_of // 2,), 0, 1 << 20) % (room + 1)
    sizes = sizes.at[source_of].add(-passed).at[receiver].add(passed)
    items = jnp.searchsorted(jnp.cumsum(sizes), jnp.arange(rows * top), side="right").astype(jnp.int32)
    grid = items.reshape(top, rows).T
    grid = grid[jax.random.permutation(jax.random.fold_in(own, 1), rows)]
    rotation = jax.random.randint(jax.random.fold_in(own, 2), (rows, 1), 0, top)
    return jnp.take_along_axis(grid, (jnp.arange(top)[None, :] + rotation) % top, axis=1)


def shares(count, total, reach, skew, full):
    weights = [(1 << 20) // math.isqrt(grade ** skew) + 1 for grade in range(1, count + 1)]
    largest = reach if full else min(reach, max(-(-total // count), total * weights[0] // sum(weights)))
    least = 1 if total - largest >= count - 1 else 0
    counts, rest = [largest] + [least] * (count - 1), total - largest - least * (count - 1)
    while rest > 0:
        candidates = [i for i in range(1, count) if counts[i] < largest] or [i for i in range(1, count) if counts[i] < reach]
        mass, budget = sum([weights[i] for i in candidates]), rest
        for i in candidates:
            addition = min(reach - counts[i], max(1, budget * weights[i] // mass), rest)
            counts[i] = counts[i] + addition
            rest = rest - addition
    return np.array(counts)


def scatter_about(stream_key, dims, scale, most, shards=(), held_as=jnp.bfloat16):
    gain = level_of(stream_key, dims, shards, -0.22, 0.18) if shards else 1.0
    drawn = jax.random.normal(stream_key, dims, jnp.float32) * scale * gain
    return jnp.minimum(jnp.maximum(drawn, -most), most).astype(held_as)


def setup_inputs(seed: int = 0) -> dict:
    splits = jax.random.split(jax.random.key(seed), 14)
    mix_query = draw_mix_query(jax.random.fold_in(splits[13], 71), 0)
    mix_key = draw_mix_key(jax.random.fold_in(splits[13], 71), 0)
    mix_value = scatter_about(splits[2], (SEQ, HEADS * VD), 1.0, 6.0, ((0, 4), (1, 8)))
    head_lambda = jnp.clip(0.3 + 0.5 * jax.random.uniform(splits[3], (HEADS,), jnp.float32) ** level_of(splits[3], (HEADS,), ((0, 8),), -0.2, 0.2), 0.3, 0.8)
    head_gain = jnp.clip(1.0 + 0.18 * jax.random.normal(splits[4], (VD,), jnp.float32), 0.1, 1.9)
    out_weight = scatter_about(splits[5], (HEADS * VD, D), (HEADS * VD) ** -0.5, 0.125, ((0, 8),))
    moe_input = scatter_about(splits[6], (TOKENS_B, D), 1.0, 6.0, ((0, 32),))
    moe_gain = jnp.clip(1.0 + 0.18 * jax.random.normal(splits[7], (D,), jnp.float32), 0.1, 1.9)
    expert_ids_keys = jax.random.split(jax.random.fold_in(splits[8], 1), TOKENS_B // ROWS_B)
    expert_ids_turns = jax.random.permutation(jax.random.fold_in(splits[8], 3), TOKENS_B // ROWS_B)
    expert_ids = jax.vmap(lambda own, number: assign_block(jax.random.fold_in(splits[8], 2), own, number, ROWS_B, EXPERTS, TOP, CAP, 2))(expert_ids_keys, expert_ids_turns).reshape((TOKENS_B, TOP))
    route_weight = jnp.clip(jnp.exp(math.log(1.0) - 1.609438 * jax.random.uniform(splits[9], (TOKENS_B, TOP), jnp.float32) ** level_of(splits[9], (TOKENS_B, TOP), ((0, 32),), -0.2, 0.2)), 0.2, 1.0)
    gate_weight = scatter_about(splits[10], (EXPERTS, D, FF), D ** -0.5, 0.125, ((0, 4), (2, 8)))
    up_weight = scatter_about(splits[11], (EXPERTS, D, FF), D ** -0.5, 0.125, ((0, 4), (2, 8)))
    down_weight = scatter_about(splits[12], (EXPERTS, FF, D), FF ** -0.5, 0.09375, ((0, 4), (1, 8)))
    return dict(mix_query=mix_query, mix_key=mix_key, mix_value=mix_value, head_lambda=head_lambda, head_gain=head_gain, out_weight=out_weight, moe_input=moe_input, moe_gain=moe_gain, expert_ids=expert_ids, route_weight=route_weight, gate_weight=gate_weight, up_weight=up_weight, down_weight=down_weight)


epsilon = 1e-06
rotary_base = 10000.0

def norm_rows(values, scales):
    square_mean = lax.optimization_barrier(jnp.mean(values * values, axis=-1, keepdims=True))
    return values * lax.rsqrt(square_mean + epsilon) * scales

def rotate(values, positions):
    half_dim = values.shape[-1] // 2
    frequency = rotary_base ** (-jnp.arange(half_dim, dtype=jnp.float32) * 2.0 / values.shape[-1])
    angles = positions.astype(jnp.float32)[:, None] * frequency[None, :]
    layout = (values.shape[0],) + (1,) * (values.ndim - 2) + (half_dim,)
    cosine = jnp.cos(angles).reshape(layout)
    sine_table = jnp.sin(angles).reshape(layout)
    leading = values[..., :half_dim]
    trailing = values[..., half_dim:]
    return jnp.concatenate([leading * cosine - trailing * sine_table, trailing * cosine + leading * sine_table], axis=-1)

def head_attention(members, head_gain):
    queries, keys, values, lambdas = members
    length = queries.shape[0]
    step_rows = math.gcd(length, 1024)
    blocks = length // step_rows

    def one_query_block(block_index):
        row_start = (block_index * step_rows).astype(jnp.int32)
        query_block = lax.dynamic_slice_in_dim(queries, row_start, step_rows, 0).astype(jnp.float32)
        query_pos = row_start + jnp.arange(step_rows, dtype=jnp.int32)

        def scores_of(key_index):
            key_start = (key_index * step_rows).astype(jnp.int32)
            key_block = lax.dynamic_slice_in_dim(keys, key_start, step_rows, 0).astype(jnp.float32)
            scores = jnp.einsum('qpd,kpd->pqk', query_block, key_block)
            key_pos = key_start + jnp.arange(step_rows, dtype=jnp.int32)
            visible = key_pos[None, :] <= query_pos[:, None]
            return (scores, visible[None, :, :], key_start)

        def find_max(key_index, running_max):
            scores, visible, unused = scores_of(key_index)
            return jnp.maximum(running_max, lax.optimization_barrier(jnp.max(jnp.where(visible, scores, -jnp.inf), axis=-1)))
        running_max = lax.fori_loop(0, block_index + 1, find_max, jnp.full((2, step_rows), -jnp.inf, jnp.float32))

        def accumulate(key_index, loop_state):
            totals, weighted = loop_state
            scores, visible, key_start = scores_of(key_index)
            expo = jnp.where(visible, jnp.exp(scores - running_max[:, :, None]), 0.0)
            rounded = lax.optimization_barrier(expo.astype(jnp.bfloat16)).astype(jnp.float32)
            value_block = lax.dynamic_slice_in_dim(values, key_start, step_rows, 0).astype(jnp.float32)
            return (totals + lax.optimization_barrier(jnp.sum(expo, axis=-1)), weighted + jnp.einsum('pqk,ke->pqe', rounded, value_block))
        initial = (jnp.zeros((2, step_rows), jnp.float32), jnp.zeros((2, step_rows, VD), jnp.float32))
        totals, weighted = lax.fori_loop(0, block_index + 1, accumulate, initial)
        combined_heads = weighted[0] / totals[0][:, None] - lambdas * weighted[1] / totals[1][:, None]
        return norm_rows(combined_heads, head_gain).astype(jnp.bfloat16)
    outputs = lax.map(one_query_block, jnp.arange(blocks, dtype=jnp.int32))
    return outputs.reshape(length, VD)

def mixer_half(mix_query, mix_key, mix_value, head_lambda, head_gain, out_weight):
    length = mix_query.shape[0]
    positions = jnp.arange(length, dtype=jnp.int32)
    queries = rotate(mix_query.astype(jnp.float32).reshape(length, HEADS, 2, HD), positions) * HD ** (-0.5)
    queries = lax.optimization_barrier(queries.astype(jnp.bfloat16))
    keys = rotate(mix_key.astype(jnp.float32).reshape(length, HEADS, 2, HD), positions)
    keys = lax.optimization_barrier(keys.astype(jnp.bfloat16))
    values = mix_value.reshape(length, HEADS, VD)

    def one_head(members):
        return head_attention(members, head_gain)
    heads_out = lax.map(one_head, (jnp.transpose(queries, (1, 0, 2, 3)), jnp.transpose(keys, (1, 0, 2, 3)), jnp.transpose(values, (1, 0, 2)), head_lambda))
    head_rows = jnp.transpose(heads_out, (1, 0, 2)).reshape(length, HEADS * VD)
    group_cols = HEADS_DEV * VD

    def add_group(group_index, totals):
        col_start = (group_index * group_cols).astype(jnp.int32)
        columns = lax.dynamic_slice_in_dim(head_rows, col_start, group_cols, 1)
        weight_rows = lax.dynamic_slice_in_dim(out_weight, col_start, group_cols, 0)
        partial_value = jnp.dot(columns, weight_rows, preferred_element_type=jnp.float32).astype(jnp.bfloat16)
        return totals + lax.optimization_barrier(partial_value).astype(jnp.float32)
    totals = lax.fori_loop(0, N_TP, add_group, jnp.zeros((length, D), jnp.float32))
    return totals.astype(jnp.bfloat16)

def experts_half(moe_input, moe_gain, expert_ids, route_weight, gate_weight, up_weight, down_weight):
    tokens = moe_input.shape[0]
    experts = gate_weight.shape[0]
    device_blocks = tokens // ROWS_B
    limit = device_blocks * CAP
    normed = norm_rows(moe_input.astype(jnp.float32), moe_gain).astype(jnp.bfloat16)
    normed = lax.optimization_barrier(normed)
    flat_ids = expert_ids.reshape(device_blocks, ROWS_B * TOP)
    member = (flat_ids[:, :, None] == jnp.arange(experts, dtype=jnp.int32)[None, None, :]).astype(jnp.int32)
    slot_rank = lax.optimization_barrier(jnp.sum(member * (jnp.cumsum(member, axis=1) - 1), axis=-1))
    destination = (jnp.arange(device_blocks, dtype=jnp.int32)[:, None] * CAP + slot_rank).reshape(tokens, TOP)

    def run_expert(expert_index, totals):
        routed = expert_ids == expert_index
        where_to = jnp.where(routed, destination, limit).astype(jnp.int32)
        buffer = jnp.zeros((limit, D), jnp.bfloat16)
        for choice_index in range(TOP):
            buffer = buffer.at[where_to[:, choice_index]].set(normed, mode='drop')
        gate_act = jnp.dot(buffer, gate_weight[expert_index], preferred_element_type=jnp.float32)
        upper = jnp.dot(buffer, up_weight[expert_index], preferred_element_type=jnp.float32)
        hidden = (jax.nn.silu(gate_act) * upper).astype(jnp.bfloat16)
        hidden = lax.optimization_barrier(hidden)
        down_here = down_weight[expert_index]

        def add_block(block_index, expert_out):
            col_start = (block_index * FF_DEV).astype(jnp.int32)
            columns = lax.dynamic_slice_in_dim(hidden, col_start, FF_DEV, 1)
            weight_rows = lax.dynamic_slice_in_dim(down_here, col_start, FF_DEV, 0)
            partial_value = jnp.dot(columns, weight_rows, preferred_element_type=jnp.float32).astype(jnp.bfloat16)
            return expert_out + lax.optimization_barrier(partial_value).astype(jnp.float32)
        expert_out = lax.fori_loop(0, N_TP, add_block, jnp.zeros((limit, D), jnp.float32)).astype(jnp.bfloat16)
        expert_out = lax.optimization_barrier(expert_out)
        for choice_index in range(TOP):
            picked = expert_out[jnp.minimum(where_to[:, choice_index], limit - 1)].astype(jnp.float32)
            contribution = route_weight[:, choice_index][:, None] * picked
            totals = totals + jnp.where(routed[:, choice_index][:, None], contribution, 0.0)
        return totals
    totals = lax.fori_loop(0, experts, run_expert, jnp.zeros((tokens, D), jnp.float32))
    return totals.astype(jnp.bfloat16)

def reference(mix_query, mix_key, mix_value, head_lambda, head_gain, out_weight, moe_input, moe_gain, expert_ids, route_weight, gate_weight, up_weight, down_weight):
    mix_output = mixer_half(mix_query, mix_key, mix_value, head_lambda, head_gain, out_weight)
    moe_output = experts_half(moe_input, moe_gain, expert_ids, route_weight, gate_weight, up_weight, down_weight)
    return (mix_output, moe_output)
```

```python
import math

import jax
import jax.numpy as jnp
from jax import lax
from jax.experimental import pallas as pl
from jax.experimental.pallas import tpu as pltpu
from jax.sharding import PartitionSpec as P

epsilon = 1e-06
rotary_base = 10000.0
far_below = -1e30


def norm_rows(values, scales):
    square_mean = jnp.mean(values * values, axis=-1, keepdims=True)
    return values * lax.rsqrt(square_mean + epsilon) * scales


def rotate(values, positions):
    half_dim = values.shape[-1] // 2
    frequency = rotary_base ** (-jnp.arange(half_dim, dtype=jnp.float32) * 2.0 / values.shape[-1])
    angles = positions.astype(jnp.float32)[:, None] * frequency[None, :]
    layout = (values.shape[0],) + (1,) * (values.ndim - 2) + (half_dim,)
    cosine = jnp.cos(angles).reshape(layout)
    sine_table = jnp.sin(angles).reshape(layout)
    leading = values[..., :half_dim]
    trailing = values[..., half_dim:]
    return jnp.concatenate(
        [leading * cosine - trailing * sine_table, trailing * cosine + leading * sine_table],
        axis=-1,
    )


def attend_block(attention_state, key_rows, value_rows, key_pos, queries, query_pos):
    running_max, totals, weighted = attention_state
    scores = jnp.einsum("qhpd,khpd->hpqk", queries, key_rows, preferred_element_type=jnp.float32)
    visible = (key_pos[None, :] <= query_pos[:, None])[None, None, :, :]
    new_max = jnp.maximum(running_max, jnp.max(jnp.where(visible, scores, far_below), axis=-1))
    expo = jnp.where(visible, jnp.exp(scores - new_max[..., None]), 0.0)
    shrink = jnp.exp(running_max - new_max)
    totals = totals * shrink + jnp.sum(expo, axis=-1)
    weighted = weighted * shrink[..., None] + jnp.einsum(
        "hpqk,khe->hpqe", expo.astype(jnp.bfloat16), value_rows, preferred_element_type=jnp.float32
    )
    return (new_max, totals, weighted)


def fold_keys(attention_state, stacked, queries, query_pos, query_last):
    heads_here = queries.shape[1]
    head_size = queries.shape[3]
    number = stacked.shape[0]
    step_rows = math.gcd(number, 1024)
    key_cols = heads_here * 2 * head_size

    def one_block(block_index, running):
        row_begin = block_index * step_rows
        key_block = lax.dynamic_slice_in_dim(stacked, row_begin, step_rows, 0)
        key_rows = key_block[:, :key_cols].reshape(step_rows, heads_here, 2, head_size)
        value_rows = key_block[:, key_cols:].reshape(step_rows, heads_here, -1)
        key_pos = row_begin + jnp.arange(step_rows, dtype=jnp.int32)

        def update(unchanged):
            return attend_block(unchanged, key_rows, value_rows, key_pos, queries, query_pos)

        def keep(unchanged):
            return unchanged

        return lax.cond(jnp.min(key_pos) > query_last, keep, update, running)

    return lax.fori_loop(0, number // step_rows, one_block, attention_state)

MESH = pl.DeviceIdType.MESH
core_count = 2
weight_parts = 3
lane_count = 128


def greet(peers):
    barrier = pltpu.get_barrier_semaphore()
    for peer in peers:
        pl.semaphore_signal(barrier, inc=1, device_id=peer, device_id_type=MESH)
    pl.semaphore_wait(barrier, len(peers))


def places(planes):
    shard, column = lax.axis_index("ep"), lax.axis_index("tp")
    level, core = column // core_count, column % core_count

    def column_at(offset):
        return lax.rem(level + offset, planes) * core_count + core

    across_x = shard + 1 - 2 * lax.rem(shard, 2)
    across_y = lax.rem(shard + 2, 4)
    shards = (shard, across_x, across_y, lax.rem(across_x + 2, 4))
    return shards, column, core, column_at


def pushed(source, target, sems, index, peer):
    return pltpu.make_async_remote_copy(
        src_ref=source,
        dst_ref=target,
        send_sem=sems.at[(0,) + index],
        recv_sem=sems.at[(1,) + index],
        device_id=peer,
        device_id_type=MESH,
    )


def layer_kernel(
    planes, own, gate_in, up_in, down_in, queries, stacked, mix_in, lambdas, gain, out, mix_out,
    keyed, mix_weight, highest, totals, weighted, head_rows, mix_parts, mix_twins, mix_all,
    held, gate, up, down, parts, twins, x_part, y_part, x_all, y_all, z_all, kept,
    kv_sem, mp_sem, mz_sem, load_sem, az_sem, ax_sem, ay_sem, afx_sem, afy_sem, ap_sem,
    p_sem, fx_sem, fy_sem, x_sem, y_sem, z_sem,
):
    shards, column, core, column_at = places(planes)
    shard, across_x, across_y, across = shards
    other = 1 - core
    twin = (shard, column + 1 - 2 * core)
    x_peer, y_peer = (across_x, column), (across_y, column)
    rows, width = out.shape
    half = rows // 2
    wide = jnp.float32
    z_peers = {step: (shard, column_at(step)) for step in range(1, planes)}
    loads = [
        pltpu.make_async_copy(source, target, load_sem.at[at])
        for at, (source, target) in enumerate(
            [
                (own, held.at[0, 0, core]),
                (gate_in, gate),
                (up_in, up),
                (down_in, down),
                (mix_in, mix_weight),
                (stacked, keyed.at[0]),
            ]
        )
    ]
    for load in loads:
        load.start()
    greet([twin, x_peer, y_peer] + list(z_peers.values()))
    sent = []

    def push(*copy_parts):
        copy = pushed(*copy_parts)
        copy.start()
        sent.append(copy)

    def landed(block, sems, index):
        pushed(block, block, sems, index, twin).wait_recv()

    push(stacked, keyed.at[1], kv_sem, (0,), x_peer)
    push(stacked, keyed.at[2], kv_sem, (1,), y_peer)
    for step in range(1, planes):
        push(own, held.at[step, 0, core], az_sem, (step,), z_peers[step])

    def spread(step):
        block = held.at[step, 0, core]
        if step:
            landed(block, az_sem, (step,))
        source = block if step else own
        push(source, held.at[step, 1, core], ax_sem, (step,), x_peer)
        push(source, held.at[step, 2, core], ay_sem, (step,), y_peer)
        push(source, block, ap_sem, (step, 0), twin)

    def forward(step):
        across_block = held.at[step, 3, core]
        block = held.at[step, 1, core]
        landed(block, ax_sem, (step,))
        push(block.at[:half], across_block.at[:half], afy_sem, (step,), y_peer)
        push(block, block, ap_sem, (step, 1), twin)
        block = held.at[step, 2, core]
        landed(block, ay_sem, (step,))
        push(block.at[half:], across_block.at[half:], afx_sem, (step,), x_peer)
        push(block, block, ap_sem, (step, 2), twin)

    def finish(step):
        block = held.at[step, 3, core]
        landed(block.at[:half], afy_sem, (step,))
        landed(block.at[half:], afx_sem, (step,))
        push(block, block, ap_sem, (step, 3), twin)

    lane_expert = lax.broadcasted_iota(jnp.int32, (1, lane_count), 1) // weight_parts

    def compute(step):
        for which in range(4):
            landed(held.at[step, which, other], ap_sem, (step, which))

        def one_part(turn, carry):
            which = jnp.where(turn == 0, 3, jnp.where(turn == 3, 0, turn))
            block = held[step, which].reshape(core_count * rows, width + lane_count)
            lanes = jnp.where(lane_expert == shard, block[:, width:].astype(wide), 0.0)
            weights = jnp.sum(lanes, axis=1, keepdims=True)
            token_rows = block[:, :width]
            gate_act = jnp.dot(token_rows, gate[...], preferred_element_type=wide)
            upper = jnp.dot(token_rows, up[...], preferred_element_type=wide)
            hidden = (gate_act / (1.0 + jnp.exp(-gate_act)) * upper).astype(own.dtype)
            result = jnp.dot(hidden, down[...], preferred_element_type=wide)
            result = (result * weights).astype(own.dtype)
            parts[step, which] = result.reshape(core_count, rows, width)
            part_copy(step, which).start()
            return carry

        lax.fori_loop(0, 4, one_part, 0)
        for which in range(4):
            sent.append(part_copy(step, which))

    def part_copy(step, which):
        return pushed(
            parts.at[step, which, other], twins.at[step, which], p_sem, (step, which), twin
        )

    def pair(step, which):
        landed(twins.at[step, which], p_sem, (step, which))
        return parts[step, which, core].astype(wide) + twins[step, which].astype(wide)

    def narrow(values):
        return values.astype(own.dtype)

    def first(step):
        twins[step, 3] = narrow(pair(step, 3))
        push(twins.at[step, 3, :half], x_part.at[step], fx_sem, (step,), x_peer)
        push(twins.at[step, 3, half:], y_part.at[step], fy_sem, (step,), y_peer)

    def second(step):
        total = pair(step, 1)
        landed(y_part.at[step], fy_sem, (step,))
        twins[step, 1, :half] = narrow(total[:half])
        twins[step, 1, half:] = narrow(total[half:] + y_part[step].astype(wide))
        push(twins.at[step, 1], x_all.at[step], x_sem, (step,), x_peer)
        total = pair(step, 2)
        landed(x_part.at[step], fx_sem, (step,))
        twins[step, 2, :half] = narrow(total[:half] + x_part[step].astype(wide))
        twins[step, 2, half:] = narrow(total[half:])
        push(twins.at[step, 2], y_all.at[step], y_sem, (step,), y_peer)

    def third(step):
        total = pair(step, 0)
        landed(x_all.at[step], x_sem, (step,))
        landed(y_all.at[step], y_sem, (step,))
        total = total + x_all[step].astype(wide) + y_all[step].astype(wide)
        if step:
            twins[step, 0] = narrow(total)
            push(twins.at[step, 0], z_all.at[step], z_sem, (step,), z_peers[planes - step])
        else:
            kept[...] = total

    seq_rows, key_cols = keyed.shape[1], queries.shape[1] // 2
    heads_here = lambdas.shape[0]
    value_size = gain.shape[1]
    pair_size = key_cols // heads_here
    key_half = seq_rows // 2

    def attend(which, diagonal):
        for unit in range(2 * heads_here):
            head = unit // 2
            scores = lax.dot_general(
                queries[:, unit * pair_size : (unit + 1) * pair_size],
                keyed[which, :, head * pair_size : (head + 1) * pair_size],
                (((1,), (1,)), ((), ())),
                preferred_element_type=wide,
            )
            if diagonal:
                key_pos = lax.broadcasted_iota(jnp.int32, scores.shape, 1)
                query_pos = lax.broadcasted_iota(jnp.int32, scores.shape, 0)
                scores = jnp.where(key_pos <= query_pos, scores, far_below)
            top = jnp.max(scores, axis=1, keepdims=True)
            if not diagonal:
                top = jnp.maximum(top, highest[unit, :, :1])
            expo = jnp.exp(scores - top)
            total = jnp.sum(expo, axis=1, keepdims=True)
            first_col = key_cols + head * value_size
            value = jnp.dot(
                narrow(expo),
                keyed[which, :, first_col : first_col + value_size],
                preferred_element_type=wide,
            )
            if not diagonal:
                shrink = jnp.exp(highest[unit, :, :1] - top)
                total = total + totals[unit, :, :1] * shrink
                value = value + weighted[unit] * shrink
            highest[unit] = jnp.broadcast_to(top, highest.shape[1:])
            totals[unit] = jnp.broadcast_to(total, totals.shape[1:])
            weighted[unit] = value

    def attend_across(which):
        across_shard = (shard, across_x, across_y, across)[which]

        @pl.when(across_shard < shard)
        def _():
            attend(which, False)

    def project():
        for head in range(heads_here):
            first_map = weighted[2 * head] / totals[2 * head]
            second_map = weighted[2 * head + 1] / totals[2 * head + 1]
            combined = first_map - lambdas[head : head + 1] * second_map
            cols = slice(head * value_size, (head + 1) * value_size)
            head_rows[:, cols] = narrow(norm_rows(combined, gain[...]))

        def one_plane(plane, carry):
            plane_rows = head_rows[pl.ds(plane * core_count * rows, core_count * rows), :]
            result = jnp.dot(plane_rows, mix_weight[...], preferred_element_type=wide)
            mix_parts[plane] = narrow(result).reshape(core_count, rows, width)
            return carry

        lax.fori_loop(0, planes, one_plane, 0)
        push(mix_parts.at[:, other], mix_twins, mp_sem, (0,), twin)

    level = column // core_count

    def mix_pair(step):
        plane = lax.rem(level + step, planes)
        return plane, mix_parts[plane, core].astype(wide) + mix_twins[plane].astype(wide)

    def mix_send():
        landed(mix_twins, mp_sem, (0,))
        for step in range(1, planes):
            plane, total = mix_pair(step)
            mix_twins[plane] = narrow(total)
            push(mix_twins.at[plane], mix_all.at[step], mz_sem, (step,), z_peers[step])

    def mix_finish():
        total = mix_pair(0)[1]
        for step in range(1, planes):
            landed(mix_all.at[step], mz_sem, (step,))
            total = total + mix_all[step].astype(wide)
        mix_out[...] = narrow(total)

    spread(0)
    loads[5].wait()
    attend(0, True)
    spread(1)
    forward(0)
    landed(keyed.at[1], kv_sem, (0,))
    push(keyed.at[1, :key_half], keyed.at[3, :key_half], kv_sem, (2,), y_peer)
    landed(keyed.at[2], kv_sem, (1,))
    push(keyed.at[2, key_half:], keyed.at[3, key_half:], kv_sem, (3,), x_peer)
    spread(2)
    attend_across(1)
    attend_across(2)
    forward(1)
    spread(3)
    finish(0)
    for load in loads[:5]:
        load.wait()
    compute(0)
    landed(keyed.at[3, :key_half], kv_sem, (2,))
    landed(keyed.at[3, key_half:], kv_sem, (3,))
    attend_across(3)
    project()
    forward(2)
    mix_send()
    finish(1)
    compute(1)
    forward(3)
    first(1)
    finish(2)
    compute(2)
    first(2)
    first(0)
    second(1)
    finish(3)
    compute(3)
    first(3)
    second(2)
    third(1)
    second(3)
    third(2)
    second(0)
    third(3)
    third(0)
    mix_finish()
    total = kept[...]
    for step in range(1, planes):
        landed(z_all.at[step], z_sem, (step,))
        total = total + z_all[step].astype(wide)
    out[...] = narrow(total)
    for copy in sent:
        copy.wait_send()


def run_layer(
    payload, gate_weight, up_weight, down_weight, queries, stacked, mix_weight, lambdas, gain,
    column_count,
):
    planes = column_count // core_count
    rows = payload.shape[0]
    width = down_weight.shape[1]
    kind = payload.dtype

    def room(*sizes):
        return pltpu.VMEM(sizes, kind)

    one = pltpu.SemaphoreType.DMA((2, planes))
    four = pltpu.SemaphoreType.DMA((2, planes, 4))
    anywhere = pl.BlockSpec(memory_space=pl.ANY)
    near = pl.BlockSpec(memory_space=pltpu.VMEM)
    seq_rows = queries.shape[0]
    state = pltpu.VMEM((2 * lambdas.shape[0], seq_rows, gain.shape[1]), jnp.float32)
    return pl.pallas_call(
        lambda *refs: layer_kernel(planes, *refs),
        out_shape=[jax.ShapeDtypeStruct((rows, width), kind)] * 2,
        in_specs=[near, anywhere, anywhere, anywhere, near, near, anywhere, near, near],
        out_specs=[near, near],
        scratch_shapes=[
            room(4, *stacked.shape),
            room(*mix_weight.shape),
            state,
            state,
            state,
            room(seq_rows, mix_weight.shape[0]),
            room(planes, core_count, rows, width),
            room(planes, rows, width),
            room(planes, rows, width),
            room(planes, 4, core_count, rows, payload.shape[1]),
            room(*gate_weight.shape),
            room(*up_weight.shape),
            room(*down_weight.shape),
            room(planes, 4, core_count, rows, width),
            room(planes, 4, rows, width),
            room(planes, rows // 2, width),
            room(planes, rows // 2, width),
            room(planes, rows, width),
            room(planes, rows, width),
            room(planes, rows, width),
            pltpu.VMEM((rows, width), jnp.float32),
            pltpu.SemaphoreType.DMA((2, 4)),
            pltpu.SemaphoreType.DMA((2, 1)),
            one,
            pltpu.SemaphoreType.DMA((6,)),
            one, one, one, one, one, four, four, one, one, one, one, one,
        ],
        compiler_params=pltpu.CompilerParams(
            collective_id=0, has_side_effects=True, vmem_limit_bytes=62 * 1024 * 1024
        ),
        cost_estimate=pl.CostEstimate(flops=0, bytes_accessed=240000000, transcendentals=0),
        name="run_layer",
    )(
        payload, gate_weight, up_weight, down_weight, queries, stacked, mix_weight, lambdas, gain
    )


def token_payload(moe_input, moe_gain, expert_ids, route_weight):
    normed = norm_rows(moe_input.astype(jnp.float32), moe_gain).astype(jnp.bfloat16)
    lane_expert = jnp.arange(lane_count, dtype=jnp.int32) // weight_parts
    lane_part = jnp.arange(lane_count, dtype=jnp.int32) % weight_parts
    spread = jnp.sum(
        jnp.where(expert_ids[:, :, None] == lane_expert, route_weight[:, :, None], 0.0), axis=1
    )
    high = lax.reduce_precision(spread, 8, 7)
    middle = lax.reduce_precision(spread - high, 8, 7)
    low = spread - high - middle
    lanes = jnp.where(lane_part == 0, high, jnp.where(lane_part == 1, middle, low))
    return jnp.concatenate([normed, lanes.astype(jnp.bfloat16)], axis=1)


def experts_exchanged(
    moe_input, moe_gain, expert_ids, route_weight, gate_weight, up_weight, down_weight
):
    ep_size = lax.axis_size("ep")
    rows_b = moe_input.shape[0]
    top_count = expert_ids.shape[1]
    exp_here = gate_weight.shape[0]
    experts = exp_here * ep_size
    slot_count = 3 * rows_b * top_count // (2 * experts)
    normed = norm_rows(moe_input.astype(jnp.float32), moe_gain).astype(jnp.bfloat16)
    flat_ids = expert_ids.reshape(rows_b * top_count)
    member = (flat_ids[:, None] == jnp.arange(experts, dtype=jnp.int32)[None, :]).astype(jnp.int32)
    slot_rank = jnp.sum(member * (jnp.cumsum(member, axis=0) - 1), axis=1)
    target = (slot_rank * experts + flat_ids).reshape(rows_b, top_count)
    selector = (
        jnp.transpose(target)[:, :, None]
        == jnp.arange(slot_count * experts, dtype=jnp.int32)[None, None, :]
    ).astype(jnp.bfloat16)
    dispatched = jnp.einsum(
        "krs,rd->sd", selector, normed, preferred_element_type=jnp.float32
    ).astype(jnp.bfloat16)
    outgoing = dispatched.reshape(1, slot_count, experts, -1)
    arrived = lax.all_to_all(outgoing, "ep", split_axis=2, concat_axis=0, tiled=True)
    expert_rows = arrived.reshape(ep_size * slot_count, exp_here, -1)
    row_block = lax.all_gather(expert_rows, "tp", axis=0, tiled=True)
    gate_act = jnp.einsum(
        "mxd,xdf->mxf", row_block, gate_weight, preferred_element_type=jnp.float32
    )
    upper = jnp.einsum("mxd,xdf->mxf", row_block, up_weight, preferred_element_type=jnp.float32)
    hidden = (jax.nn.silu(gate_act) * upper).astype(jnp.bfloat16)
    row_block = hidden
    expert_sum = lax.psum_scatter(
        jnp.einsum(
            "mxf,xfd->mxd", row_block, down_weight, preferred_element_type=jnp.float32
        ).astype(jnp.bfloat16),
        "tp",
        scatter_dimension=0,
        tiled=True,
    )
    returning = expert_sum.reshape(ep_size, slot_count, exp_here, -1)
    returned = lax.all_to_all(returning, "ep", split_axis=0, concat_axis=2, tiled=True)
    results = returned.reshape(slot_count * experts, -1)
    chosen = jnp.einsum("krs,sd->krd", selector, results, preferred_element_type=jnp.float32)
    combined = jnp.sum(chosen * jnp.transpose(route_weight)[:, :, None], axis=0)
    return combined.astype(jnp.bfloat16)


def body(
    mix_query,
    mix_key,
    mix_value,
    head_lambda,
    head_gain,
    out_weight,
    moe_input,
    moe_gain,
    expert_ids,
    route_weight,
    gate_weight,
    up_weight,
    down_weight,
):
    seq_rows = mix_query.shape[0]
    heads_here = head_lambda.shape[0]
    head_size = mix_query.shape[1] // (2 * heads_here)
    value_size = mix_value.shape[1] // heads_here
    ep_size = lax.axis_size("ep")
    my_shard = lax.axis_index("ep")
    query_pos = my_shard * seq_rows + jnp.arange(seq_rows, dtype=jnp.int32)
    queries = rotate(
        mix_query.astype(jnp.float32).reshape(seq_rows, heads_here, 2, head_size), query_pos
    )
    queries = (queries * head_size ** (-0.5)).astype(jnp.bfloat16)
    rotated_keys = rotate(
        mix_key.astype(jnp.float32).reshape(seq_rows, heads_here, 2, head_size), query_pos
    )
    rotated_keys = rotated_keys.astype(jnp.bfloat16).reshape(seq_rows, heads_here * 2 * head_size)
    stacked = jnp.concatenate([rotated_keys, mix_value], axis=1)
    square = ep_size == 4 and lax.axis_size("tp") % core_count == 0
    if square and gate_weight.shape[0] == 1 and weight_parts * ep_size <= lane_count:
        map_of = jnp.eye(2, dtype=jnp.bfloat16)[None, None, :, :, None]
        apart = (queries[:, :, :, None, :] * map_of).reshape(seq_rows, -1)
        moe_output, mix_output = run_layer(
            token_payload(moe_input, moe_gain, expert_ids, route_weight),
            gate_weight[0],
            up_weight[0],
            down_weight[0],
            apart,
            stacked,
            out_weight,
            jnp.broadcast_to(head_lambda[:, None], (heads_here, value_size)),
            head_gain[None, :],
            lax.axis_size("tp"),
        )
        return (mix_output, moe_output)
    query_last = jnp.max(query_pos)
    initial = (
        jnp.full((heads_here, 2, seq_rows), far_below, jnp.float32),
        jnp.zeros((heads_here, 2, seq_rows), jnp.float32),
        jnp.zeros((heads_here, 2, seq_rows, value_size), jnp.float32),
    )
    attention_state = fold_keys(
        initial, lax.all_gather(stacked, "ep", axis=0, tiled=True), queries, query_pos, query_last
    )
    running_max, totals, weighted = attention_state
    lambdas = head_lambda[:, None, None]
    combined_heads = (
        weighted[:, 0] / totals[:, 0][..., None]
        - lambdas * weighted[:, 1] / totals[:, 1][..., None]
    )
    combined_heads = norm_rows(combined_heads, head_gain).astype(jnp.bfloat16)
    head_rows = jnp.transpose(combined_heads, (1, 0, 2)).reshape(seq_rows, heads_here * value_size)
    mix_partial = jnp.dot(head_rows, out_weight, preferred_element_type=jnp.float32)
    mix_sum = lax.psum_scatter(
        mix_partial.astype(jnp.bfloat16), "tp", scatter_dimension=0, tiled=True
    )
    moe_args = (
        moe_input, moe_gain, expert_ids, route_weight, gate_weight, up_weight, down_weight
    )
    return (mix_sum, experts_exchanged(*moe_args))


def solution(mesh):
    return jax.shard_map(
        body,
        mesh=mesh,
        in_specs=(
            P("ep", "tp"),
            P("ep", "tp"),
            P("ep", "tp"),
            P("tp"),
            P(),
            P("tp", None),
            P(("ep", "tp"), None),
            P(),
            P(("ep", "tp"), None),
            P(("ep", "tp"), None),
            P("ep", None, "tp"),
            P("ep", None, "tp"),
            P("ep", "tp", None),
        ),
        out_specs=(P(("ep", "tp"), None), P(("ep", "tp"), None)),
        check_vma=False,
    )
```

```python
import math

import jax
import jax.numpy as jnp
import numpy as np
from jax import lax
from jax.experimental import pallas as pl
from jax.experimental.pallas import tpu as pltpu
from jax.sharding import PartitionSpec as P

epsilon = 1e-06
rotary_base = 10000.0
far_below = -1e30


def norm_rows(values, scales):
    square_mean = jnp.mean(values * values, axis=-1, keepdims=True)
    return values * lax.rsqrt(square_mean + epsilon) * scales


def rotate(values, positions):
    half_dim = values.shape[-1] // 2
    frequency = rotary_base ** (-jnp.arange(half_dim, dtype=jnp.float32) * 2.0 / values.shape[-1])
    angles = positions.astype(jnp.float32)[:, None] * frequency[None, :]
    layout = (values.shape[0],) + (1,) * (values.ndim - 2) + (half_dim,)
    cosine = jnp.cos(angles).reshape(layout)
    sine_table = jnp.sin(angles).reshape(layout)
    leading = values[..., :half_dim]
    trailing = values[..., half_dim:]
    return jnp.concatenate(
        [leading * cosine - trailing * sine_table, trailing * cosine + leading * sine_table],
        axis=-1,
    )


def attend_block(attention_state, key_rows, value_rows, key_pos, queries, query_pos):
    running_max, totals, weighted = attention_state
    scores = jnp.einsum("qhpd,khpd->hpqk", queries, key_rows, preferred_element_type=jnp.float32)
    visible = (key_pos[None, :] <= query_pos[:, None])[None, None, :, :]
    new_max = jnp.maximum(running_max, jnp.max(jnp.where(visible, scores, far_below), axis=-1))
    expo = jnp.where(visible, jnp.exp(scores - new_max[..., None]), 0.0)
    shrink = jnp.exp(running_max - new_max)
    totals = totals * shrink + jnp.sum(expo, axis=-1)
    weighted = weighted * shrink[..., None] + jnp.einsum(
        "hpqk,khe->hpqe", expo.astype(jnp.bfloat16), value_rows, preferred_element_type=jnp.float32
    )
    return (new_max, totals, weighted)


def fold_keys(attention_state, stacked, queries, query_pos, query_last):
    heads_here = queries.shape[1]
    head_size = queries.shape[3]
    number = stacked.shape[0]
    step_rows = math.gcd(number, 1024)
    key_cols = heads_here * 2 * head_size

    def one_block(block_index, running):
        row_begin = block_index * step_rows
        key_block = lax.dynamic_slice_in_dim(stacked, row_begin, step_rows, 0)
        key_rows = key_block[:, :key_cols].reshape(step_rows, heads_here, 2, head_size)
        value_rows = key_block[:, key_cols:].reshape(step_rows, heads_here, -1)
        key_pos = row_begin + jnp.arange(step_rows, dtype=jnp.int32)

        def update(unchanged):
            return attend_block(unchanged, key_rows, value_rows, key_pos, queries, query_pos)

        def keep(unchanged):
            return unchanged

        return lax.cond(jnp.min(key_pos) > query_last, keep, update, running)

    return lax.fori_loop(0, number // step_rows, one_block, attention_state)

MESH = pl.DeviceIdType.MESH
core_count = 2
weight_parts = 3
lane_count = 128


def greet(peers):
    barrier = pltpu.get_barrier_semaphore()
    for peer in peers:
        pl.semaphore_signal(barrier, inc=1, device_id=peer, device_id_type=MESH)
    pl.semaphore_wait(barrier, len(peers))


def places(planes):
    shard, column = lax.axis_index("ep"), lax.axis_index("tp")
    level, core = column // core_count, column % core_count

    def column_at(slot):
        beside = level + 1 - 2 * lax.rem(level, 2)
        return (level, beside, lax.rem(level + 2, planes), planes - 1 - level)[slot] * core_count + core

    across_x = shard + 1 - 2 * lax.rem(shard, 2)
    across_y = lax.rem(shard + 2, 4)
    shards = (shard, across_x, across_y, lax.rem(across_x + 2, 4))
    return shards, column, core, column_at


def pushed(source, target, sems, index, peer):
    return pltpu.make_async_remote_copy(
        src_ref=source,
        dst_ref=target,
        send_sem=sems.at[(0,) + index],
        recv_sem=sems.at[(1,) + index],
        device_id=peer,
        device_id_type=MESH,
    )


def layer_kernel(
    planes, moe_in, moe_gain_in, ids_in, route_in, gate_in, up_in, down_in, query_in, key_in,
    value_in, turn_in, mix_in, lambda_in, gain_in, out, mix_out,
    moe_rows, moe_gain, ids, route, raw_query, raw_key, turns, lambdas, gain, queries,
    cosines, sines, keyed, mix_weight, highest, totals, weighted, head_rows, mix_parts, mix_twins, mix_all,
    held, gate, up, down, parts, twins, x_part, y_part, x_all, y_all, z_all, kept,
    kv_sem, mp_sem, mz_sem, load_sem, az_sem, ax_sem, ay_sem, afx_sem, afy_sem, ap_sem,
    p_sem, fx_sem, fy_sem, x_sem, y_sem, z_sem,
):
    shards, column, core, column_at = places(planes)
    shard, across_x, across_y, across = shards
    other = 1 - core
    twin = (shard, column + 1 - 2 * core)
    x_peer, y_peer = (across_x, column), (across_y, column)
    rows, width = out.shape
    half = rows // 2
    wide = jnp.float32
    far_first = (2, 3, 1)
    z_peers = {step: (shard, column_at(step)) for step in range(1, planes)}
    kind = held.dtype
    key_cols = raw_key.shape[1]
    loads = [
        pltpu.make_async_copy(source, target, load_sem.at[at])
        for at, (source, target) in enumerate(
            [
                (moe_in, moe_rows),
                (moe_gain_in, moe_gain),
                (ids_in, ids),
                (route_in, route),
                (key_in, raw_key),
                (turn_in, turns),
                (value_in, keyed.at[0, :, key_cols:]),
                (query_in, raw_query),
                (gate_in, gate),
                (up_in, up),
                (down_in, down),
                (mix_in, mix_weight),
                (lambda_in, lambdas),
                (gain_in, gain),
            ]
        )
    ]
    for load in loads:
        load.start()
    peers = [twin, x_peer, y_peer] + list(z_peers.values())
    barrier = pltpu.get_barrier_semaphore()
    for peer in peers:
        pl.semaphore_signal(barrier, inc=1, device_id=peer, device_id_type=MESH)
    for load in loads[:4]:
        load.wait()
    held[0, 0, core] = token_payload(moe_rows[...], moe_gain[...], ids[...], route[...])
    pl.semaphore_wait(barrier, len(peers))
    sent = []

    def push(*copy_parts):
        copy = pushed(*copy_parts)
        copy.start()
        sent.append(copy)

    def landed(block, sems, index):
        pushed(block, block, sems, index, twin).wait_recv()

    def send_keys():
        push(keyed.at[0], keyed.at[1], kv_sem, (0,), x_peer)
        push(keyed.at[0], keyed.at[2], kv_sem, (1,), y_peer)

    def send_planes():
        for step in far_first:
            push(held.at[0, 0, core], held.at[step, 0, core], az_sem, (step,), z_peers[step])

    def spread(step):
        block = held.at[step, 0, core]
        if step:
            landed(block, az_sem, (step,))
        if step != 1:
            push(block, held.at[step, 1, core], ax_sem, (step,), x_peer)
            push(block, held.at[step, 2, core], ay_sem, (step,), y_peer)
        push(block, block, ap_sem, (step, 0), twin)

    def relay(which, sems):
        push(held.at[0, which, core], held.at[1, which, core], sems, (1,), z_peers[1])

    def gather(which, sems):
        block = held.at[1, which, core]
        landed(block, sems, (1,))
        push(block, block, ap_sem, (1, which), twin)

    def forward(step):
        across_block = held.at[step, 3, core]
        block = held.at[step, 1, core]
        landed(block, ax_sem, (step,))
        push(block.at[:half], across_block.at[:half], afy_sem, (step,), y_peer)
        push(block, block, ap_sem, (step, 1), twin)
        block = held.at[step, 2, core]
        landed(block, ay_sem, (step,))
        push(block.at[half:], across_block.at[half:], afx_sem, (step,), x_peer)
        push(block, block, ap_sem, (step, 2), twin)
        if step == 0:
            relay(1, ax_sem)
            relay(2, ay_sem)

    def finish(step):
        block = held.at[step, 3, core]
        landed(block.at[:half], afy_sem, (step,))
        landed(block.at[half:], afx_sem, (step,))
        push(block, block, ap_sem, (step, 3), twin)
        if step == 0:
            relay(3, afx_sem)

    lane_expert = lax.broadcasted_iota(jnp.int32, (1, lane_count), 1) // weight_parts

    def compute(step):
        for which in range(4):
            landed(held.at[step, which, other], ap_sem, (step, which))

        def one_part(turn, carry):
            which = jnp.where(turn == 0, 3, jnp.where(turn == 3, 0, turn))
            block = held[step, which].reshape(core_count * rows, width + lane_count)
            lanes = jnp.where(lane_expert == shard, block[:, width:].astype(wide), 0.0)
            weights = jnp.sum(lanes, axis=1, keepdims=True)
            token_rows = block[:, :width]
            gate_act = jnp.dot(token_rows, gate[...], preferred_element_type=wide)
            upper = jnp.dot(token_rows, up[...], preferred_element_type=wide)
            hidden = (gate_act / (1.0 + jnp.exp(-gate_act)) * upper).astype(kind)
            result = jnp.dot(hidden, down[...], preferred_element_type=wide)
            result = (result * weights).astype(kind)
            parts[step, which] = result.reshape(core_count, rows, width)
            part_copy(step, which).start()
            return carry

        lax.fori_loop(0, 4, one_part, 0)
        for which in range(4):
            sent.append(part_copy(step, which))

    def part_copy(step, which):
        return pushed(
            parts.at[step, which, other], twins.at[step, which], p_sem, (step, which), twin
        )

    def pair(step, which):
        landed(twins.at[step, which], p_sem, (step, which))
        return parts[step, which, core].astype(wide) + twins[step, which].astype(wide)

    def narrow(values):
        return values.astype(kind)

    def first(step):
        twins[step, 3] = narrow(pair(step, 3))
        push(twins.at[step, 3, :half], x_part.at[step], fx_sem, (step,), x_peer)
        push(twins.at[step, 3, half:], y_part.at[step], fy_sem, (step,), y_peer)

    def second(step):
        total = pair(step, 1)
        landed(y_part.at[step], fy_sem, (step,))
        twins[step, 1, :half] = narrow(total[:half])
        twins[step, 1, half:] = narrow(total[half:] + y_part[step].astype(wide))
        push(twins.at[step, 1], x_all.at[step], x_sem, (step,), x_peer)
        total = pair(step, 2)
        landed(x_part.at[step], fx_sem, (step,))
        twins[step, 2, :half] = narrow(total[:half] + x_part[step].astype(wide))
        twins[step, 2, half:] = narrow(total[half:])
        push(twins.at[step, 2], y_all.at[step], y_sem, (step,), y_peer)

    def third(step):
        total = pair(step, 0)
        landed(x_all.at[step], x_sem, (step,))
        landed(y_all.at[step], y_sem, (step,))
        total = total + x_all[step].astype(wide) + y_all[step].astype(wide)
        if step:
            twins[step, 0] = narrow(total)
            push(twins.at[step, 0], z_all.at[step], z_sem, (step,), z_peers[step])
        else:
            kept[...] = total

    seq_rows = keyed.shape[1]
    heads_here = lambdas.shape[1]
    value_size = gain.shape[1]
    pair_size = key_cols // heads_here
    key_half = seq_rows // 2

    def wider(values):
        return jnp.broadcast_to(values, (seq_rows, value_size))

    turn_rows = seq_rows // 8
    map_size = pair_size // 2
    lane = lax.broadcasted_iota(jnp.int32, (turn_rows, pair_size), 1)
    leading = lax.rem(lane, map_size) < map_size // 2

    def rotated(source, rows_at, head, cosine, sine):
        values = source[rows_at, head * pair_size : (head + 1) * pair_size].astype(wide)
        ahead = pltpu.roll(values, pair_size - map_size // 2, 1)
        behind = pltpu.roll(values, map_size // 2, 1)
        return values * cosine + jnp.where(leading, ahead, behind) * sine

    def rotate_keys():
        def one_chunk(chunk, carry):
            rows_at = pl.ds(pl.multiple_of(chunk * turn_rows, turn_rows), turn_rows)
            place = lax.broadcasted_iota(jnp.int32, (turn_rows, pair_size), 0)
            place = place + (shard * seq_rows + chunk * turn_rows)
            angles = place.astype(wide) * turns[...]
            cosine, sine = jnp.cos(angles), jnp.sin(angles)
            sine = jnp.where(leading, -sine, sine)
            cosines[rows_at, :] = cosine
            sines[rows_at, :] = sine
            for head in range(heads_here):
                keyed[0, rows_at, head * pair_size : (head + 1) * pair_size] = narrow(
                    rotated(raw_key, rows_at, head, cosine, sine)
                )
            return carry

        lax.fori_loop(0, 8, one_chunk, 0)

    def rotate_queries():
        def one_chunk(chunk, carry):
            rows_at = pl.ds(pl.multiple_of(chunk * turn_rows, turn_rows), turn_rows)
            cosine, sine = cosines[rows_at, :], sines[rows_at, :]
            for head in range(heads_here):
                values = rotated(raw_query, rows_at, head, cosine, sine) * map_size ** (-0.5)
                for half_at in range(2):
                    unit = 2 * head + half_at
                    own_map = (lane // map_size) == half_at
                    queries[rows_at, unit * pair_size : (unit + 1) * pair_size] = narrow(
                        jnp.where(own_map, values, 0.0)
                    )
            return carry

        lax.fori_loop(0, 8, one_chunk, 0)

    def attend(which, diagonal):
        for unit in range(2 * heads_here):
            head = unit // 2
            scores = lax.dot_general(
                queries[:, unit * pair_size : (unit + 1) * pair_size],
                keyed[which, :, head * pair_size : (head + 1) * pair_size],
                (((1,), (1,)), ((), ())),
                preferred_element_type=wide,
            )
            if diagonal:
                key_pos = lax.broadcasted_iota(jnp.int32, scores.shape, 1)
                query_pos = lax.broadcasted_iota(jnp.int32, scores.shape, 0)
                scores = jnp.where(key_pos <= query_pos, scores, far_below)
            top = wider(jnp.max(scores, axis=1, keepdims=True))
            if not diagonal:
                top = jnp.maximum(top, highest[unit])
            expo = jnp.exp(scores - jnp.concatenate([top] * (seq_rows // value_size), axis=1))
            total = wider(jnp.sum(expo, axis=1, keepdims=True))
            first_col = key_cols + head * value_size
            value = jnp.dot(
                narrow(expo),
                keyed[which, :, first_col : first_col + value_size],
                preferred_element_type=wide,
            )
            if not diagonal:
                shrink = jnp.exp(highest[unit] - top)
                total = total + totals[unit] * shrink
                value = value + weighted[unit] * shrink
            highest[unit] = top
            totals[unit] = total
            weighted[unit] = value

    def attend_across(which):
        across_shard = (shard, across_x, across_y, across)[which]

        @pl.when(across_shard < shard)
        def _():
            attend(which, False)

    def project():
        for head in range(heads_here):
            first_map = weighted[2 * head] / totals[2 * head]
            second_map = weighted[2 * head + 1] / totals[2 * head + 1]
            combined = first_map - lambdas[:, head : head + 1] * second_map
            cols = slice(head * value_size, (head + 1) * value_size)
            head_rows[:, cols] = narrow(norm_rows(combined, gain[...]))

        def one_plane(plane, carry):
            plane_rows = head_rows[pl.ds(plane * core_count * rows, core_count * rows), :]
            result = jnp.dot(plane_rows, mix_weight[...], preferred_element_type=wide)
            mix_parts[plane] = narrow(result).reshape(core_count, rows, width)
            return carry

        lax.fori_loop(0, planes, one_plane, 0)
        push(mix_parts.at[:, other], mix_twins, mp_sem, (0,), twin)

    level = column // core_count

    def mix_pair(step):
        plane = column_at(step) // core_count
        return plane, mix_parts[plane, core].astype(wide) + mix_twins[plane].astype(wide)

    def mix_send():
        landed(mix_twins, mp_sem, (0,))
        for step in range(1, planes):
            plane, total = mix_pair(step)
            mix_twins[plane] = narrow(total)
            push(mix_twins.at[plane], mix_all.at[step], mz_sem, (step,), z_peers[step])

    def mix_finish():
        total = mix_pair(0)[1]
        for step in range(1, planes):
            landed(mix_all.at[step], mz_sem, (step,))
            total = total + mix_all[step].astype(wide)
        mix_out[...] = narrow(total)

    send_planes()
    spread(0)
    for load in loads[4:8]:
        load.wait()
    rotate_keys()
    send_keys()
    rotate_queries()
    attend(0, True)
    forward(0)
    landed(keyed.at[1], kv_sem, (0,))
    push(keyed.at[1, :key_half], keyed.at[3, :key_half], kv_sem, (2,), y_peer)
    landed(keyed.at[2], kv_sem, (1,))
    push(keyed.at[2, key_half:], keyed.at[3, key_half:], kv_sem, (3,), x_peer)
    spread(2)
    attend_across(1)
    attend_across(2)
    finish(0)
    for load in loads[8:]:
        load.wait()
    compute(0)
    landed(keyed.at[3, :key_half], kv_sem, (2,))
    landed(keyed.at[3, key_half:], kv_sem, (3,))
    attend_across(3)
    project()
    forward(2)
    spread(3)
    spread(1)
    mix_send()
    finish(2)
    compute(2)
    first(2)
    gather(1, ax_sem)
    forward(3)
    first(0)
    gather(2, ay_sem)
    gather(3, afx_sem)
    compute(1)
    second(2)
    finish(3)
    compute(3)
    first(3)
    first(1)
    third(2)
    second(3)
    second(1)
    third(3)
    second(0)
    third(1)
    third(0)
    mix_finish()
    total = kept[...]
    for step in range(1, planes):
        landed(z_all.at[step], z_sem, (step,))
        total = total + z_all[step].astype(wide)
    out[...] = narrow(total)
    for copy in sent:
        copy.wait_send()


def run_layer(
    moe_input, moe_gain, expert_ids, route_weight, gate_weight, up_weight, down_weight,
    mix_query, mix_key, mix_value, turns, mix_weight, lambdas, gain, column_count,
):
    planes = column_count // core_count
    rows, width = moe_input.shape
    kind = moe_input.dtype
    arrays = [
        moe_input, moe_gain, expert_ids, route_weight, gate_weight, up_weight, down_weight,
        mix_query, mix_key, mix_value, turns, mix_weight, lambdas, gain,
    ]

    def room(*sizes):
        return pltpu.VMEM(sizes, kind)

    one = pltpu.SemaphoreType.DMA((2, planes))
    four = pltpu.SemaphoreType.DMA((2, planes, 4))
    anywhere = pl.BlockSpec(memory_space=pl.ANY)
    near = pl.BlockSpec(memory_space=pltpu.VMEM)
    seq_rows, key_cols = mix_key.shape
    state = pltpu.VMEM((2 * lambdas.shape[1], seq_rows, gain.shape[1]), jnp.float32)

    def like(array):
        return pltpu.VMEM(array.shape, array.dtype)

    return pl.pallas_call(
        lambda *refs: layer_kernel(planes, *refs),
        out_shape=[pltpu.VMEM((rows, width), kind)] * 2,
        in_specs=[anywhere] * len(arrays),
        out_specs=[near, near],
        scratch_shapes=[
            like(moe_input),
            like(moe_gain),
            like(expert_ids),
            like(route_weight),
            like(mix_query),
            like(mix_key),
            like(turns),
            like(lambdas),
            like(gain),
            room(seq_rows, 2 * key_cols),
            pltpu.VMEM((seq_rows, turns.shape[1]), jnp.float32),
            pltpu.VMEM((seq_rows, turns.shape[1]), jnp.float32),
            room(4, seq_rows, key_cols + mix_value.shape[1]),
            room(*mix_weight.shape),
            state,
            state,
            state,
            room(seq_rows, mix_weight.shape[0]),
            room(planes, core_count, rows, width),
            room(planes, rows, width),
            room(planes, rows, width),
            room(planes, 4, core_count, rows, width + lane_count),
            room(*gate_weight.shape),
            room(*up_weight.shape),
            room(*down_weight.shape),
            room(planes, 4, core_count, rows, width),
            room(planes, 4, rows, width),
            room(planes, rows // 2, width),
            room(planes, rows // 2, width),
            room(planes, rows, width),
            room(planes, rows, width),
            room(planes, rows, width),
            pltpu.VMEM((rows, width), jnp.float32),
            pltpu.SemaphoreType.DMA((2, 4)),
            pltpu.SemaphoreType.DMA((2, 1)),
            one,
            pltpu.SemaphoreType.DMA((len(arrays),)),
            one, one, one, one, one, four, four, one, one, one, one, one,
        ],
        compiler_params=pltpu.CompilerParams(
            collective_id=0, has_side_effects=True, vmem_limit_bytes=62 * 1024 * 1024
        ),
        cost_estimate=pl.CostEstimate(flops=0, bytes_accessed=240000000, transcendentals=0),
        name="run_layer",
    )(*arrays)


def token_payload(moe_rows, moe_gain, expert_ids, route_weight):
    kind = moe_rows.dtype
    normed = norm_rows(moe_rows.astype(jnp.float32), moe_gain).astype(kind)
    lane = lax.broadcasted_iota(jnp.int32, (lane_count, moe_rows.shape[0]), 0)
    lane_expert, lane_part = lane // weight_parts, lax.rem(lane, weight_parts)
    spread = jnp.zeros(lane.shape, jnp.float32)
    for choice in range(expert_ids.shape[0]):
        chosen = expert_ids[choice : choice + 1, :] == lane_expert
        spread = spread + jnp.where(chosen, route_weight[choice : choice + 1, :], 0.0)
    high = spread.astype(kind).astype(jnp.float32)
    middle = (spread - high).astype(kind).astype(jnp.float32)
    low = spread - high - middle
    lanes = jnp.where(lane_part == 0, high, jnp.where(lane_part == 1, middle, low))
    return jnp.concatenate([normed, jnp.transpose(lanes).astype(kind)], axis=1)


def experts_exchanged(
    moe_input, moe_gain, expert_ids, route_weight, gate_weight, up_weight, down_weight
):
    ep_size = lax.axis_size("ep")
    rows_b = moe_input.shape[0]
    top_count = expert_ids.shape[1]
    exp_here = gate_weight.shape[0]
    experts = exp_here * ep_size
    slot_count = 3 * rows_b * top_count // (2 * experts)
    normed = norm_rows(moe_input.astype(jnp.float32), moe_gain).astype(jnp.bfloat16)
    flat_ids = expert_ids.reshape(rows_b * top_count)
    member = (flat_ids[:, None] == jnp.arange(experts, dtype=jnp.int32)[None, :]).astype(jnp.int32)
    slot_rank = jnp.sum(member * (jnp.cumsum(member, axis=0) - 1), axis=1)
    target = (slot_rank * experts + flat_ids).reshape(rows_b, top_count)
    selector = (
        jnp.transpose(target)[:, :, None]
        == jnp.arange(slot_count * experts, dtype=jnp.int32)[None, None, :]
    ).astype(jnp.bfloat16)
    dispatched = jnp.einsum(
        "krs,rd->sd", selector, normed, preferred_element_type=jnp.float32
    ).astype(jnp.bfloat16)
    outgoing = dispatched.reshape(1, slot_count, experts, -1)
    arrived = lax.all_to_all(outgoing, "ep", split_axis=2, concat_axis=0, tiled=True)
    expert_rows = arrived.reshape(ep_size * slot_count, exp_here, -1)
    row_block = lax.all_gather(expert_rows, "tp", axis=0, tiled=True)
    gate_act = jnp.einsum(
        "mxd,xdf->mxf", row_block, gate_weight, preferred_element_type=jnp.float32
    )
    upper = jnp.einsum("mxd,xdf->mxf", row_block, up_weight, preferred_element_type=jnp.float32)
    hidden = (jax.nn.silu(gate_act) * upper).astype(jnp.bfloat16)
    row_block = hidden
    expert_sum = lax.psum_scatter(
        jnp.einsum(
            "mxf,xfd->mxd", row_block, down_weight, preferred_element_type=jnp.float32
        ).astype(jnp.bfloat16),
        "tp",
        scatter_dimension=0,
        tiled=True,
    )
    returning = expert_sum.reshape(ep_size, slot_count, exp_here, -1)
    returned = lax.all_to_all(returning, "ep", split_axis=0, concat_axis=2, tiled=True)
    results = returned.reshape(slot_count * experts, -1)
    chosen = jnp.einsum("krs,sd->krd", selector, results, preferred_element_type=jnp.float32)
    combined = jnp.sum(chosen * jnp.transpose(route_weight)[:, :, None], axis=0)
    return combined.astype(jnp.bfloat16)


def body(
    mix_query,
    mix_key,
    mix_value,
    head_lambda,
    head_gain,
    out_weight,
    moe_input,
    moe_gain,
    expert_ids,
    route_weight,
    gate_weight,
    up_weight,
    down_weight,
):
    seq_rows = mix_query.shape[0]
    heads_here = head_lambda.shape[0]
    head_size = mix_query.shape[1] // (2 * heads_here)
    value_size = mix_value.shape[1] // heads_here
    ep_size = lax.axis_size("ep")
    my_shard = lax.axis_index("ep")
    tp_size = lax.axis_size("tp")
    square = ep_size == 4 and tp_size == 4 * core_count
    if square and gate_weight.shape[0] == 1 and weight_parts * ep_size <= lane_count:
        frequency = rotary_base ** (-np.arange(head_size // 2) * 2.0 / head_size)
        moe_output, mix_output = run_layer(
            moe_input,
            moe_gain[None, :],
            jnp.transpose(expert_ids),
            jnp.transpose(route_weight),
            gate_weight[0],
            up_weight[0],
            down_weight[0],
            mix_query,
            mix_key,
            mix_value,
            jnp.asarray(np.tile(frequency, 4)[None, :], jnp.float32),
            out_weight,
            head_lambda[None, :],
            head_gain[None, :],
            tp_size,
        )
        return (mix_output, moe_output)
    query_pos = my_shard * seq_rows + jnp.arange(seq_rows, dtype=jnp.int32)
    queries = rotate(
        mix_query.astype(jnp.float32).reshape(seq_rows, heads_here, 2, head_size), query_pos
    )
    queries = (queries * head_size ** (-0.5)).astype(jnp.bfloat16)
    rotated_keys = rotate(
        mix_key.astype(jnp.float32).reshape(seq_rows, heads_here, 2, head_size), query_pos
    )
    rotated_keys = rotated_keys.astype(jnp.bfloat16).reshape(seq_rows, heads_here * 2 * head_size)
    stacked = jnp.concatenate([rotated_keys, mix_value], axis=1)
    query_last = jnp.max(query_pos)
    initial = (
        jnp.full((heads_here, 2, seq_rows), far_below, jnp.float32),
        jnp.zeros((heads_here, 2, seq_rows), jnp.float32),
        jnp.zeros((heads_here, 2, seq_rows, value_size), jnp.float32),
    )
    attention_state = fold_keys(
        initial, lax.all_gather(stacked, "ep", axis=0, tiled=True), queries, query_pos, query_last
    )
    running_max, totals, weighted = attention_state
    lambdas = head_lambda[:, None, None]
    combined_heads = (
        weighted[:, 0] / totals[:, 0][..., None]
        - lambdas * weighted[:, 1] / totals[:, 1][..., None]
    )
    combined_heads = norm_rows(combined_heads, head_gain).astype(jnp.bfloat16)
    head_rows = jnp.transpose(combined_heads, (1, 0, 2)).reshape(seq_rows, heads_here * value_size)
    mix_partial = jnp.dot(head_rows, out_weight, preferred_element_type=jnp.float32)
    mix_sum = lax.psum_scatter(
        mix_partial.astype(jnp.bfloat16), "tp", scatter_dimension=0, tiled=True
    )
    moe_args = (
        moe_input, moe_gain, expert_ids, route_weight, gate_weight, up_weight, down_weight
    )
    return (mix_sum, experts_exchanged(*moe_args))


def solution(mesh):
    return jax.shard_map(
        body,
        mesh=mesh,
        in_specs=(
            P("ep", "tp"),
            P("ep", "tp"),
            P("ep", "tp"),
            P("tp"),
            P(),
            P("tp", None),
            P(("ep", "tp"), None),
            P(),
            P(("ep", "tp"), None),
            P(("ep", "tp"), None),
            P("ep", None, "tp"),
            P("ep", None, "tp"),
            P("ep", "tp", None),
        ),
        out_specs=(P(("ep", "tp"), None), P(("ep", "tp"), None)),
        check_vma=False,
    )
```

```python
import math

import jax
import jax.numpy as jnp
import numpy as np
from jax import lax
from jax.experimental import pallas as pl
from jax.experimental.pallas import tpu as pltpu
from jax.sharding import PartitionSpec as P

epsilon = 1e-06
rotary_base = 10000.0
far_below = -1e30


def norm_rows(values, scales):
    square_mean = jnp.mean(values * values, axis=-1, keepdims=True)
    return values * lax.rsqrt(square_mean + epsilon) * scales


def rotate(values, positions):
    half_dim = values.shape[-1] // 2
    frequency = rotary_base ** (-jnp.arange(half_dim, dtype=jnp.float32) * 2.0 / values.shape[-1])
    angles = positions.astype(jnp.float32)[:, None] * frequency[None, :]
    layout = (values.shape[0],) + (1,) * (values.ndim - 2) + (half_dim,)
    cosine = jnp.cos(angles).reshape(layout)
    sine_table = jnp.sin(angles).reshape(layout)
    leading = values[..., :half_dim]
    trailing = values[..., half_dim:]
    return jnp.concatenate(
        [leading * cosine - trailing * sine_table, trailing * cosine + leading * sine_table],
        axis=-1,
    )


def attend_block(attention_state, key_rows, value_rows, key_pos, queries, query_pos):
    running_max, totals, weighted = attention_state
    scores = jnp.einsum("qhpd,khpd->hpqk", queries, key_rows, preferred_element_type=jnp.float32)
    visible = (key_pos[None, :] <= query_pos[:, None])[None, None, :, :]
    new_max = jnp.maximum(running_max, jnp.max(jnp.where(visible, scores, far_below), axis=-1))
    expo = jnp.where(visible, jnp.exp(scores - new_max[..., None]), 0.0)
    shrink = jnp.exp(running_max - new_max)
    totals = totals * shrink + jnp.sum(expo, axis=-1)
    weighted = weighted * shrink[..., None] + jnp.einsum(
        "hpqk,khe->hpqe", expo.astype(jnp.bfloat16), value_rows, preferred_element_type=jnp.float32
    )
    return (new_max, totals, weighted)


def fold_keys(attention_state, stacked, queries, query_pos, query_last):
    heads_here = queries.shape[1]
    head_size = queries.shape[3]
    number = stacked.shape[0]
    step_rows = math.gcd(number, 1024)
    key_cols = heads_here * 2 * head_size

    def one_block(block_index, running):
        row_begin = block_index * step_rows
        key_block = lax.dynamic_slice_in_dim(stacked, row_begin, step_rows, 0)
        key_rows = key_block[:, :key_cols].reshape(step_rows, heads_here, 2, head_size)
        value_rows = key_block[:, key_cols:].reshape(step_rows, heads_here, -1)
        key_pos = row_begin + jnp.arange(step_rows, dtype=jnp.int32)

        def update(unchanged):
            return attend_block(unchanged, key_rows, value_rows, key_pos, queries, query_pos)

        def keep(unchanged):
            return unchanged

        return lax.cond(jnp.min(key_pos) > query_last, keep, update, running)

    return lax.fori_loop(0, number // step_rows, one_block, attention_state)

MESH = pl.DeviceIdType.MESH
core_count = 2
weight_parts = 3
lane_count = 128


def greet(peers):
    barrier = pltpu.get_barrier_semaphore()
    for peer in peers:
        pl.semaphore_signal(barrier, inc=1, device_id=peer, device_id_type=MESH)
    pl.semaphore_wait(barrier, len(peers))


def places(planes):
    shard, column = lax.axis_index("ep"), lax.axis_index("tp")
    level, core = column // core_count, column % core_count

    def column_at(slot):
        beside = level + 1 - 2 * lax.rem(level, 2)
        return (level, beside, lax.rem(level + 2, planes), planes - 1 - level)[slot] * core_count + core

    across_x = shard + 1 - 2 * lax.rem(shard, 2)
    across_y = lax.rem(shard + 2, 4)
    shards = (shard, across_x, across_y, lax.rem(across_x + 2, 4))
    return shards, column, core, column_at


def pushed(source, target, sems, index, peer):
    return pltpu.make_async_remote_copy(
        src_ref=source,
        dst_ref=target,
        send_sem=sems.at[(0,) + index],
        recv_sem=sems.at[(1,) + index],
        device_id=peer,
        device_id_type=MESH,
    )


def layer_kernel(
    planes, moe_in, moe_gain_in, ids_in, route_in, gate_in, up_in, down_in, query_in, key_in,
    value_in, turn_in, mix_in, lambda_in, gain_in, out, mix_out,
    moe_rows, moe_gain, ids, route, raw_query, raw_key, turns, lambdas, gain, queries,
    cosines, sines, keyed, mix_weight, highest, totals, weighted, head_rows, mix_parts, mix_twins, mix_all,
    held, gate, up, down, parts, twins, x_part, y_part, x_all, y_all, z_all, kept,
    kv_sem, mp_sem, mz_sem, load_sem, az_sem, ax_sem, ay_sem, afx_sem, afy_sem, ap_sem,
    p_sem, fx_sem, fy_sem, x_sem, y_sem, z_sem,
):
    shards, column, core, column_at = places(planes)
    shard, across_x, across_y, across = shards
    other = 1 - core
    twin = (shard, column + 1 - 2 * core)
    x_peer, y_peer = (across_x, column), (across_y, column)
    rows, width = out.shape
    half = rows // 2
    wide = jnp.float32
    far_first = (2, 3, 1)
    z_peers = {step: (shard, column_at(step)) for step in range(1, planes)}
    kind = held.dtype
    key_cols = raw_key.shape[1]
    loads = [
        pltpu.make_async_copy(source, target, load_sem.at[at])
        for at, (source, target) in enumerate(
            [
                (moe_in, moe_rows),
                (moe_gain_in, moe_gain),
                (ids_in, ids),
                (route_in, route),
                (key_in, raw_key),
                (turn_in, turns),
                (value_in, keyed.at[0, :, key_cols:]),
                (query_in, raw_query),
                (gate_in, gate),
                (up_in, up),
                (down_in, down),
                (mix_in, mix_weight),
                (lambda_in, lambdas),
                (gain_in, gain),
            ]
        )
    ]
    for load in loads:
        load.start()
    peers = [twin, x_peer, y_peer] + list(z_peers.values())
    barrier = pltpu.get_barrier_semaphore()
    for peer in peers:
        pl.semaphore_signal(barrier, inc=1, device_id=peer, device_id_type=MESH)
    for load in loads[:4]:
        load.wait()
    held[0, 0, core] = token_payload(moe_rows[...], moe_gain[...], ids[...], route[...])
    pl.semaphore_wait(barrier, len(peers))
    sent = []

    def push(*copy_parts):
        copy = pushed(*copy_parts)
        copy.start()
        sent.append(copy)

    def landed(block, sems, index):
        pushed(block, block, sems, index, twin).wait_recv()

    def send_keys():
        push(keyed.at[0], keyed.at[1], kv_sem, (0,), x_peer)
        push(keyed.at[0], keyed.at[2], kv_sem, (1,), y_peer)

    def send_planes():
        for step in far_first:
            push(held.at[0, 0, core], held.at[step, 0, core], az_sem, (step,), z_peers[step])

    def spread(step):
        block = held.at[step, 0, core]
        if step:
            landed(block, az_sem, (step,))
        if step != 1:
            for turn, (part, late) in enumerate((("low", "high"), ("high", "low"))):
                for sems, which, peer, name in (
                    (ax_sem, 1, x_peer, part),
                    (ay_sem, 2, y_peer, late),
                ):
                    target = held.at[step, which, core]
                    push(cut(block, name), cut(target, name), sems, (step, turn), peer)
        push(block, block, ap_sem, (step, 0), twin)

    def cut(block, name):
        return block.at[:half] if name == "low" else block.at[half:]

    def relay(which, sems, index):
        push(held.at[0, which, core], held.at[1, which, core], sems, index, z_peers[1])

    def gather(which, sems, index):
        block = held.at[1, which, core]
        landed(block, sems, index)
        push(block, block, ap_sem, (1, which), twin)

    def forward(step):
        across_block = held.at[step, 3, core]
        block = held.at[step, 1, core]
        landed(block.at[:half], ax_sem, (step, 0))
        push(block.at[:half], across_block.at[:half], afy_sem, (step,), y_peer)
        block = held.at[step, 2, core]
        landed(block.at[half:], ay_sem, (step, 0))
        push(block.at[half:], across_block.at[half:], afx_sem, (step,), x_peer)

    def settle(step):
        block = held.at[step, 1, core]
        landed(block.at[half:], ax_sem, (step, 1))
        push(block, block, ap_sem, (step, 1), twin)
        block = held.at[step, 2, core]
        landed(block.at[:half], ay_sem, (step, 1))
        push(block, block, ap_sem, (step, 2), twin)
        if step == 0:
            relay(1, ax_sem, (1, 0))
            relay(2, ay_sem, (1, 0))

    def finish(step):
        block = held.at[step, 3, core]
        landed(block.at[:half], afy_sem, (step,))
        landed(block.at[half:], afx_sem, (step,))
        push(block, block, ap_sem, (step, 3), twin)
        if step == 0:
            relay(3, afx_sem, (1,))

    lane_expert = lax.broadcasted_iota(jnp.int32, (1, lane_count), 1) // weight_parts

    def compute(step):
        for which in range(4):
            landed(held.at[step, which, other], ap_sem, (step, which))

        def one_part(turn, carry):
            which = jnp.where(turn == 0, 3, jnp.where(turn == 3, 0, turn))
            block = held[step, which].reshape(core_count * rows, width + lane_count)
            lanes = jnp.where(lane_expert == shard, block[:, width:].astype(wide), 0.0)
            weights = jnp.sum(lanes, axis=1, keepdims=True)
            token_rows = block[:, :width]
            gate_act = jnp.dot(token_rows, gate[...], preferred_element_type=wide)
            upper = jnp.dot(token_rows, up[...], preferred_element_type=wide)
            hidden = (gate_act / (1.0 + jnp.exp(-gate_act)) * upper).astype(kind)
            result = jnp.dot(hidden, down[...], preferred_element_type=wide)
            result = (result * weights).astype(kind)
            parts[step, which] = result.reshape(core_count, rows, width)
            part_copy(step, which).start()
            return carry

        lax.fori_loop(0, 4, one_part, 0)
        for which in range(4):
            sent.append(part_copy(step, which))

    def part_copy(step, which):
        return pushed(
            parts.at[step, which, other], twins.at[step, which], p_sem, (step, which), twin
        )

    def sums(step, which, begin, end):
        mine = parts[step, which, core, begin:end].astype(wide)
        return mine + twins[step, which, begin:end].astype(wide)

    def pair(step, which):
        landed(twins.at[step, which], p_sem, (step, which))
        return sums(step, which, 0, rows)

    def narrow(values):
        return values.astype(kind)

    def first(step):
        twins[step, 3] = narrow(pair(step, 3))
        push(twins.at[step, 3, :half], x_part.at[step], fx_sem, (step,), x_peer)
        push(twins.at[step, 3, half:], y_part.at[step], fy_sem, (step,), y_peer)

    def early(step):
        for which in (1, 2):
            landed(twins.at[step, which], p_sem, (step, which))
        twins[step, 1, :half] = narrow(sums(step, 1, 0, half))
        push(twins.at[step, 1, :half], x_all.at[step, :half], x_sem, (step, 0), x_peer)
        twins[step, 2, half:] = narrow(sums(step, 2, half, rows))
        push(twins.at[step, 2, half:], y_all.at[step, half:], y_sem, (step, 0), y_peer)

    def second(step):
        total = sums(step, 1, half, rows)
        landed(y_part.at[step], fy_sem, (step,))
        twins[step, 1, half:] = narrow(total + y_part[step].astype(wide))
        push(twins.at[step, 1, half:], x_all.at[step, half:], x_sem, (step, 1), x_peer)
        total = sums(step, 2, 0, half)
        landed(x_part.at[step], fx_sem, (step,))
        twins[step, 2, :half] = narrow(total + x_part[step].astype(wide))
        push(twins.at[step, 2, :half], y_all.at[step, :half], y_sem, (step, 1), y_peer)

    def third(step):
        total = pair(step, 0)
        for part in range(2):
            landed(x_all.at[step, part * half : (part + 1) * half], x_sem, (step, part))
            landed(y_all.at[step, (1 - part) * half : (2 - part) * half], y_sem, (step, part))
        total = total + x_all[step].astype(wide) + y_all[step].astype(wide)
        if step:
            twins[step, 0] = narrow(total)
            push(twins.at[step, 0], z_all.at[step], z_sem, (step,), z_peers[step])
        else:
            kept[...] = total

    seq_rows = keyed.shape[1]
    heads_here = lambdas.shape[1]
    value_size = gain.shape[1]
    pair_size = key_cols // heads_here
    key_half = seq_rows // 2

    def wider(values):
        return jnp.broadcast_to(values, (seq_rows, value_size))

    turn_rows = seq_rows // 8
    map_size = pair_size // 2
    lane = lax.broadcasted_iota(jnp.int32, (turn_rows, pair_size), 1)
    leading = lax.rem(lane, map_size) < map_size // 2

    def rotated(source, rows_at, head, cosine, sine):
        values = source[rows_at, head * pair_size : (head + 1) * pair_size].astype(wide)
        ahead = pltpu.roll(values, pair_size - map_size // 2, 1)
        behind = pltpu.roll(values, map_size // 2, 1)
        return values * cosine + jnp.where(leading, ahead, behind) * sine

    def rotate_keys():
        def one_chunk(chunk, carry):
            rows_at = pl.ds(pl.multiple_of(chunk * turn_rows, turn_rows), turn_rows)
            place = lax.broadcasted_iota(jnp.int32, (turn_rows, pair_size), 0)
            place = place + (shard * seq_rows + chunk * turn_rows)
            angles = place.astype(wide) * turns[...]
            cosine, sine = jnp.cos(angles), jnp.sin(angles)
            sine = jnp.where(leading, -sine, sine)
            cosines[rows_at, :] = cosine
            sines[rows_at, :] = sine
            for head in range(heads_here):
                keyed[0, rows_at, head * pair_size : (head + 1) * pair_size] = narrow(
                    rotated(raw_key, rows_at, head, cosine, sine)
                )
            return carry

        lax.fori_loop(0, 8, one_chunk, 0)

    def rotate_queries():
        def one_chunk(chunk, carry):
            rows_at = pl.ds(pl.multiple_of(chunk * turn_rows, turn_rows), turn_rows)
            cosine, sine = cosines[rows_at, :], sines[rows_at, :]
            for head in range(heads_here):
                values = rotated(raw_query, rows_at, head, cosine, sine) * map_size ** (-0.5)
                for half_at in range(2):
                    unit = 2 * head + half_at
                    own_map = (lane // map_size) == half_at
                    queries[rows_at, unit * pair_size : (unit + 1) * pair_size] = narrow(
                        jnp.where(own_map, values, 0.0)
                    )
            return carry

        lax.fori_loop(0, 8, one_chunk, 0)

    def attend(which, diagonal):
        for unit in range(2 * heads_here):
            head = unit // 2
            scores = lax.dot_general(
                queries[:, unit * pair_size : (unit + 1) * pair_size],
                keyed[which, :, head * pair_size : (head + 1) * pair_size],
                (((1,), (1,)), ((), ())),
                preferred_element_type=wide,
            )
            if diagonal:
                key_pos = lax.broadcasted_iota(jnp.int32, scores.shape, 1)
                query_pos = lax.broadcasted_iota(jnp.int32, scores.shape, 0)
                scores = jnp.where(key_pos <= query_pos, scores, far_below)
            top = wider(jnp.max(scores, axis=1, keepdims=True))
            if not diagonal:
                top = jnp.maximum(top, highest[unit])
            expo = jnp.exp(scores - jnp.concatenate([top] * (seq_rows // value_size), axis=1))
            total = wider(jnp.sum(expo, axis=1, keepdims=True))
            first_col = key_cols + head * value_size
            value = jnp.dot(
                narrow(expo),
                keyed[which, :, first_col : first_col + value_size],
                preferred_element_type=wide,
            )
            if not diagonal:
                shrink = jnp.exp(highest[unit] - top)
                total = total + totals[unit] * shrink
                value = value + weighted[unit] * shrink
            highest[unit] = top
            totals[unit] = total
            weighted[unit] = value

    def attend_across(which):
        across_shard = (shard, across_x, across_y, across)[which]

        @pl.when(across_shard < shard)
        def _():
            attend(which, False)

    def project():
        for head in range(heads_here):
            first_map = weighted[2 * head] / totals[2 * head]
            second_map = weighted[2 * head + 1] / totals[2 * head + 1]
            combined = first_map - lambdas[:, head : head + 1] * second_map
            cols = slice(head * value_size, (head + 1) * value_size)
            head_rows[:, cols] = narrow(norm_rows(combined, gain[...]))

        def one_plane(plane, carry):
            plane_rows = head_rows[pl.ds(plane * core_count * rows, core_count * rows), :]
            result = jnp.dot(plane_rows, mix_weight[...], preferred_element_type=wide)
            mix_parts[plane] = narrow(result).reshape(core_count, rows, width)
            return carry

        lax.fori_loop(0, planes, one_plane, 0)
        push(mix_parts.at[:, other], mix_twins, mp_sem, (0,), twin)

    level = column // core_count

    def mix_pair(step):
        plane = column_at(step) // core_count
        return plane, mix_parts[plane, core].astype(wide) + mix_twins[plane].astype(wide)

    def mix_send():
        landed(mix_twins, mp_sem, (0,))
        for step in range(1, planes):
            plane, total = mix_pair(step)
            mix_twins[plane] = narrow(total)
            push(mix_twins.at[plane], mix_all.at[step], mz_sem, (step,), z_peers[step])

    def mix_finish():
        total = mix_pair(0)[1]
        for step in range(1, planes):
            landed(mix_all.at[step], mz_sem, (step,))
            total = total + mix_all[step].astype(wide)
        mix_out[...] = narrow(total)

    send_planes()
    spread(0)
    for load in loads[4:8]:
        load.wait()
    rotate_keys()
    send_keys()
    rotate_queries()
    attend(0, True)
    forward(0)
    settle(0)
    landed(keyed.at[1], kv_sem, (0,))
    push(keyed.at[1, :key_half], keyed.at[3, :key_half], kv_sem, (2,), y_peer)
    landed(keyed.at[2], kv_sem, (1,))
    push(keyed.at[2, key_half:], keyed.at[3, key_half:], kv_sem, (3,), x_peer)
    finish(0)
    spread(2)
    attend_across(1)
    attend_across(2)
    landed(keyed.at[3, :key_half], kv_sem, (2,))
    landed(keyed.at[3, key_half:], kv_sem, (3,))
    attend_across(3)
    for load in loads[8:]:
        load.wait()
    project()
    forward(2)
    mix_send()
    gather(1, ax_sem, (1, 0))
    settle(2)
    spread(3)
    finish(2)
    forward(3)
    compute(2)
    first(2)
    finish(3)
    spread(1)
    gather(2, ay_sem, (1, 0))
    early(2)
    settle(3)
    gather(3, afx_sem, (1,))
    second(2)
    compute(3)
    first(3)
    early(3)
    third(2)
    compute(1)
    first(1)
    second(3)
    compute(0)
    early(1)
    third(3)
    second(1)
    first(0)
    early(0)
    third(1)
    second(0)
    third(0)
    mix_finish()
    total = kept[...]
    for step in range(1, planes):
        landed(z_all.at[step], z_sem, (step,))
        total = total + z_all[step].astype(wide)
    out[...] = narrow(total)
    for copy in sent:
        copy.wait_send()


def run_layer(
    moe_input, moe_gain, expert_ids, route_weight, gate_weight, up_weight, down_weight,
    mix_query, mix_key, mix_value, turns, mix_weight, lambdas, gain, column_count,
):
    planes = column_count // core_count
    rows, width = moe_input.shape
    kind = moe_input.dtype
    arrays = [
        moe_input, moe_gain, expert_ids, route_weight, gate_weight, up_weight, down_weight,
        mix_query, mix_key, mix_value, turns, mix_weight, lambdas, gain,
    ]

    def room(*sizes):
        return pltpu.VMEM(sizes, kind)

    one = pltpu.SemaphoreType.DMA((2, planes))
    two = pltpu.SemaphoreType.DMA((2, planes, 2))
    four = pltpu.SemaphoreType.DMA((2, planes, 4))
    anywhere = pl.BlockSpec(memory_space=pl.ANY)
    near = pl.BlockSpec(memory_space=pltpu.VMEM)
    seq_rows, key_cols = mix_key.shape
    state = pltpu.VMEM((2 * lambdas.shape[1], seq_rows, gain.shape[1]), jnp.float32)

    def like(array):
        return pltpu.VMEM(array.shape, array.dtype)

    return pl.pallas_call(
        lambda *refs: layer_kernel(planes, *refs),
        out_shape=[pltpu.VMEM((rows, width), kind)] * 2,
        in_specs=[anywhere] * len(arrays),
        out_specs=[near, near],
        scratch_shapes=[
            like(moe_input),
            like(moe_gain),
            like(expert_ids),
            like(route_weight),
            like(mix_query),
            like(mix_key),
            like(turns),
            like(lambdas),
            like(gain),
            room(seq_rows, 2 * key_cols),
            pltpu.VMEM((seq_rows, turns.shape[1]), jnp.float32),
            pltpu.VMEM((seq_rows, turns.shape[1]), jnp.float32),
            room(4, seq_rows, key_cols + mix_value.shape[1]),
            room(*mix_weight.shape),
            state,
            state,
            state,
            room(seq_rows, mix_weight.shape[0]),
            room(planes, core_count, rows, width),
            room(planes, rows, width),
            room(planes, rows, width),
            room(planes, 4, core_count, rows, width + lane_count),
            room(*gate_weight.shape),
            room(*up_weight.shape),
            room(*down_weight.shape),
            room(planes, 4, core_count, rows, width),
            room(planes, 4, rows, width),
            room(planes, rows // 2, width),
            room(planes, rows // 2, width),
            room(planes, rows, width),
            room(planes, rows, width),
            room(planes, rows, width),
            pltpu.VMEM((rows, width), jnp.float32),
            pltpu.SemaphoreType.DMA((2, 4)),
            pltpu.SemaphoreType.DMA((2, 1)),
            one,
            pltpu.SemaphoreType.DMA((len(arrays),)),
            one, two, two, one, one, four, four, one, one, two, two, one,
        ],
        compiler_params=pltpu.CompilerParams(
            collective_id=0, has_side_effects=True, vmem_limit_bytes=62 * 1024 * 1024
        ),
        cost_estimate=pl.CostEstimate(flops=0, bytes_accessed=240000000, transcendentals=0),
        name="run_layer",
    )(*arrays)


def token_payload(moe_rows, moe_gain, expert_ids, route_weight):
    kind = moe_rows.dtype
    normed = norm_rows(moe_rows.astype(jnp.float32), moe_gain).astype(kind)
    lane = lax.broadcasted_iota(jnp.int32, (lane_count, moe_rows.shape[0]), 0)
    lane_expert, lane_part = lane // weight_parts, lax.rem(lane, weight_parts)
    spread = jnp.zeros(lane.shape, jnp.float32)
    for choice in range(expert_ids.shape[0]):
        chosen = expert_ids[choice : choice + 1, :] == lane_expert
        spread = spread + jnp.where(chosen, route_weight[choice : choice + 1, :], 0.0)
    high = spread.astype(kind).astype(jnp.float32)
    middle = (spread - high).astype(kind).astype(jnp.float32)
    low = spread - high - middle
    lanes = jnp.where(lane_part == 0, high, jnp.where(lane_part == 1, middle, low))
    return jnp.concatenate([normed, jnp.transpose(lanes).astype(kind)], axis=1)


def experts_exchanged(
    moe_input, moe_gain, expert_ids, route_weight, gate_weight, up_weight, down_weight
):
    ep_size = lax.axis_size("ep")
    rows_b = moe_input.shape[0]
    top_count = expert_ids.shape[1]
    exp_here = gate_weight.shape[0]
    experts = exp_here * ep_size
    slot_count = 3 * rows_b * top_count // (2 * experts)
    normed = norm_rows(moe_input.astype(jnp.float32), moe_gain).astype(jnp.bfloat16)
    flat_ids = expert_ids.reshape(rows_b * top_count)
    member = (flat_ids[:, None] == jnp.arange(experts, dtype=jnp.int32)[None, :]).astype(jnp.int32)
    slot_rank = jnp.sum(member * (jnp.cumsum(member, axis=0) - 1), axis=1)
    target = (slot_rank * experts + flat_ids).reshape(rows_b, top_count)
    selector = (
        jnp.transpose(target)[:, :, None]
        == jnp.arange(slot_count * experts, dtype=jnp.int32)[None, None, :]
    ).astype(jnp.bfloat16)
    dispatched = jnp.einsum(
        "krs,rd->sd", selector, normed, preferred_element_type=jnp.float32
    ).astype(jnp.bfloat16)
    outgoing = dispatched.reshape(1, slot_count, experts, -1)
    arrived = lax.all_to_all(outgoing, "ep", split_axis=2, concat_axis=0, tiled=True)
    expert_rows = arrived.reshape(ep_size * slot_count, exp_here, -1)
    row_block = lax.all_gather(expert_rows, "tp", axis=0, tiled=True)
    gate_act = jnp.einsum(
        "mxd,xdf->mxf", row_block, gate_weight, preferred_element_type=jnp.float32
    )
    upper = jnp.einsum("mxd,xdf->mxf", row_block, up_weight, preferred_element_type=jnp.float32)
    hidden = (jax.nn.silu(gate_act) * upper).astype(jnp.bfloat16)
    row_block = hidden
    expert_sum = lax.psum_scatter(
        jnp.einsum(
            "mxf,xfd->mxd", row_block, down_weight, preferred_element_type=jnp.float32
        ).astype(jnp.bfloat16),
        "tp",
        scatter_dimension=0,
        tiled=True,
    )
    returning = expert_sum.reshape(ep_size, slot_count, exp_here, -1)
    returned = lax.all_to_all(returning, "ep", split_axis=0, concat_axis=2, tiled=True)
    results = returned.reshape(slot_count * experts, -1)
    chosen = jnp.einsum("krs,sd->krd", selector, results, preferred_element_type=jnp.float32)
    combined = jnp.sum(chosen * jnp.transpose(route_weight)[:, :, None], axis=0)
    return combined.astype(jnp.bfloat16)


def body(
    mix_query,
    mix_key,
    mix_value,
    head_lambda,
    head_gain,
    out_weight,
    moe_input,
    moe_gain,
    expert_ids,
    route_weight,
    gate_weight,
    up_weight,
    down_weight,
):
    seq_rows = mix_query.shape[0]
    heads_here = head_lambda.shape[0]
    head_size = mix_query.shape[1] // (2 * heads_here)
    value_size = mix_value.shape[1] // heads_here
    ep_size = lax.axis_size("ep")
    my_shard = lax.axis_index("ep")
    tp_size = lax.axis_size("tp")
    square = ep_size == 4 and tp_size == 4 * core_count
    if square and gate_weight.shape[0] == 1 and weight_parts * ep_size <= lane_count:
        frequency = rotary_base ** (-np.arange(head_size // 2) * 2.0 / head_size)
        moe_output, mix_output = run_layer(
            moe_input,
            moe_gain[None, :],
            jnp.transpose(expert_ids),
            jnp.transpose(route_weight),
            gate_weight[0],
            up_weight[0],
            down_weight[0],
            mix_query,
            mix_key,
            mix_value,
            jnp.asarray(np.tile(frequency, 4)[None, :], jnp.float32),
            out_weight,
            head_lambda[None, :],
            head_gain[None, :],
            tp_size,
        )
        return (mix_output, moe_output)
    query_pos = my_shard * seq_rows + jnp.arange(seq_rows, dtype=jnp.int32)
    queries = rotate(
        mix_query.astype(jnp.float32).reshape(seq_rows, heads_here, 2, head_size), query_pos
    )
    queries = (queries * head_size ** (-0.5)).astype(jnp.bfloat16)
    rotated_keys = rotate(
        mix_key.astype(jnp.float32).reshape(seq_rows, heads_here, 2, head_size), query_pos
    )
    rotated_keys = rotated_keys.astype(jnp.bfloat16).reshape(seq_rows, heads_here * 2 * head_size)
    stacked = jnp.concatenate([rotated_keys, mix_value], axis=1)
    query_last = jnp.max(query_pos)
    initial = (
        jnp.full((heads_here, 2, seq_rows), far_below, jnp.float32),
        jnp.zeros((heads_here, 2, seq_rows), jnp.float32),
        jnp.zeros((heads_here, 2, seq_rows, value_size), jnp.float32),
    )
    attention_state = fold_keys(
        initial, lax.all_gather(stacked, "ep", axis=0, tiled=True), queries, query_pos, query_last
    )
    running_max, totals, weighted = attention_state
    lambdas = head_lambda[:, None, None]
    combined_heads = (
        weighted[:, 0] / totals[:, 0][..., None]
        - lambdas * weighted[:, 1] / totals[:, 1][..., None]
    )
    combined_heads = norm_rows(combined_heads, head_gain).astype(jnp.bfloat16)
    head_rows = jnp.transpose(combined_heads, (1, 0, 2)).reshape(seq_rows, heads_here * value_size)
    mix_partial = jnp.dot(head_rows, out_weight, preferred_element_type=jnp.float32)
    mix_sum = lax.psum_scatter(
        mix_partial.astype(jnp.bfloat16), "tp", scatter_dimension=0, tiled=True
    )
    moe_args = (
        moe_input, moe_gain, expert_ids, route_weight, gate_weight, up_weight, down_weight
    )
    return (mix_sum, experts_exchanged(*moe_args))


def solution(mesh):
    return jax.shard_map(
        body,
        mesh=mesh,
        in_specs=(
            P("ep", "tp"),
            P("ep", "tp"),
            P("ep", "tp"),
            P("tp"),
            P(),
            P("tp", None),
            P(("ep", "tp"), None),
            P(),
            P(("ep", "tp"), None),
            P(("ep", "tp"), None),
            P("ep", None, "tp"),
            P("ep", None, "tp"),
            P("ep", "tp", None),
        ),
        out_specs=(P(("ep", "tp"), None), P(("ep", "tp"), None)),
        check_vma=False,
    )
```

```python
import math

import jax
import jax.numpy as jnp
import numpy as np
from jax import lax
from jax.experimental import pallas as pl
from jax.experimental.pallas import tpu as pltpu
from jax.sharding import PartitionSpec as P

epsilon = 1e-06
rotary_base = 10000.0
far_below = -1e30


def norm_rows(values, scales):
    square_mean = jnp.mean(values * values, axis=-1, keepdims=True)
    return values * lax.rsqrt(square_mean + epsilon) * scales


def rotate(values, positions):
    half_dim = values.shape[-1] // 2
    frequency = rotary_base ** (-jnp.arange(half_dim, dtype=jnp.float32) * 2.0 / values.shape[-1])
    angles = positions.astype(jnp.float32)[:, None] * frequency[None, :]
    layout = (values.shape[0],) + (1,) * (values.ndim - 2) + (half_dim,)
    cosine = jnp.cos(angles).reshape(layout)
    sine_table = jnp.sin(angles).reshape(layout)
    leading = values[..., :half_dim]
    trailing = values[..., half_dim:]
    return jnp.concatenate(
        [leading * cosine - trailing * sine_table, trailing * cosine + leading * sine_table],
        axis=-1,
    )


def attend_block(attention_state, key_rows, value_rows, key_pos, queries, query_pos):
    running_max, totals, weighted = attention_state
    scores = jnp.einsum("qhpd,khpd->hpqk", queries, key_rows, preferred_element_type=jnp.float32)
    visible = (key_pos[None, :] <= query_pos[:, None])[None, None, :, :]
    new_max = jnp.maximum(running_max, jnp.max(jnp.where(visible, scores, far_below), axis=-1))
    expo = jnp.where(visible, jnp.exp(scores - new_max[..., None]), 0.0)
    shrink = jnp.exp(running_max - new_max)
    totals = totals * shrink + jnp.sum(expo, axis=-1)
    weighted = weighted * shrink[..., None] + jnp.einsum(
        "hpqk,khe->hpqe", expo.astype(jnp.bfloat16), value_rows, preferred_element_type=jnp.float32
    )
    return (new_max, totals, weighted)


def fold_keys(attention_state, stacked, queries, query_pos, query_last):
    heads_here = queries.shape[1]
    head_size = queries.shape[3]
    number = stacked.shape[0]
    step_rows = math.gcd(number, 1024)
    key_cols = heads_here * 2 * head_size

    def one_block(block_index, running):
        row_begin = block_index * step_rows
        key_block = lax.dynamic_slice_in_dim(stacked, row_begin, step_rows, 0)
        key_rows = key_block[:, :key_cols].reshape(step_rows, heads_here, 2, head_size)
        value_rows = key_block[:, key_cols:].reshape(step_rows, heads_here, -1)
        key_pos = row_begin + jnp.arange(step_rows, dtype=jnp.int32)

        def update(unchanged):
            return attend_block(unchanged, key_rows, value_rows, key_pos, queries, query_pos)

        def keep(unchanged):
            return unchanged

        return lax.cond(jnp.min(key_pos) > query_last, keep, update, running)

    return lax.fori_loop(0, number // step_rows, one_block, attention_state)

MESH = pl.DeviceIdType.MESH
core_count = 2
share_rows = 8


def greet(peers):
    barrier = pltpu.get_barrier_semaphore()
    for peer in peers:
        pl.semaphore_signal(barrier, inc=1, device_id=peer, device_id_type=MESH)
    pl.semaphore_wait(barrier, len(peers))


def places(planes):
    shard, column = lax.axis_index("ep"), lax.axis_index("tp")
    level, core = column // core_count, column % core_count

    def column_at(slot):
        beside = level + 1 - 2 * lax.rem(level, 2)
        return (level, beside, lax.rem(level + 2, planes), planes - 1 - level)[slot] * core_count + core

    across_x = shard + 1 - 2 * lax.rem(shard, 2)
    across_y = lax.rem(shard + 2, 4)
    shards = (shard, across_x, across_y, lax.rem(across_x + 2, 4))
    return shards, column, core, column_at


def pushed(source, target, sems, index, peer):
    return pltpu.make_async_remote_copy(
        src_ref=source,
        dst_ref=target,
        send_sem=sems.at[(0,) + index],
        recv_sem=sems.at[(1,) + index],
        device_id=peer,
        device_id_type=MESH,
    )


def layer_kernel(
    planes, moe_in, moe_gain_in, ids_in, route_in, gate_in, up_in, down_in, query_in, key_in,
    value_in, turn_in, mix_in, lambda_in, gain_in, out, mix_out,
    moe_rows, moe_gain, ids, route, raw_query, raw_key, turns, lambdas, gain, queries,
    cosines, sines, keyed, mix_weight, highest, totals, weighted, head_rows, mix_parts, mix_twins, mix_all,
    held, gate, up, down, parts, twins, x_part, y_part, x_all, y_all, z_all, kept, shares, wz_sem, ws_sem,
    kv_sem, mp_sem, mz_sem, load_sem, az_sem, ax_sem, ay_sem, afx_sem, afy_sem, ap_sem,
    p_sem, fx_sem, fy_sem, x_sem, y_sem, z_sem,
):
    shards, column, core, column_at = places(planes)
    shard, across_x, across_y, across = shards
    other = 1 - core
    twin = (shard, column + 1 - 2 * core)
    x_peer, y_peer = (across_x, column), (across_y, column)
    rows, width = out.shape
    half = rows // 2
    wide = jnp.float32
    far_first = (2, 3, 1)
    z_peers = {step: (shard, column_at(step)) for step in range(1, planes)}
    kind = held.dtype
    key_cols = raw_key.shape[1]
    loads = [
        pltpu.make_async_copy(source, target, load_sem.at[at])
        for at, (source, target) in enumerate(
            [
                (moe_in, moe_rows),
                (moe_gain_in, moe_gain),
                (ids_in, ids),
                (route_in, route),
                (key_in, raw_key),
                (turn_in, turns),
                (value_in, keyed.at[0, :, key_cols:]),
                (query_in, raw_query),
                (gate_in, gate),
                (up_in, up),
                (down_in, down),
                (mix_in, mix_weight),
                (lambda_in, lambdas),
                (gain_in, gain),
            ]
        )
    ]
    for load in loads:
        load.start()
    peers = [twin, x_peer, y_peer] + list(z_peers.values())
    barrier = pltpu.get_barrier_semaphore()
    for peer in peers:
        pl.semaphore_signal(barrier, inc=1, device_id=peer, device_id_type=MESH)
    for load in loads[:4]:
        load.wait()
    held[0, 0, core] = norm_rows(moe_rows[...].astype(wide), moe_gain[...]).astype(kind)
    shares[0, 0, core] = route_shares(ids[...], route[...], core)
    pl.semaphore_wait(barrier, len(peers))
    sent = []

    def push(*copy_parts):
        copy = pushed(*copy_parts)
        copy.start()
        sent.append(copy)

    def landed(block, sems, index):
        pushed(block, block, sems, index, twin).wait_recv()

    def send_keys():
        push(keyed.at[0], keyed.at[1], kv_sem, (0,), x_peer)
        push(keyed.at[0], keyed.at[2], kv_sem, (1,), y_peer)

    def send_planes():
        for step in far_first:
            push(held.at[0, 0, core], held.at[step, 0, core], az_sem, (step,), z_peers[step])

    def spread(step):
        block = held.at[step, 0, core]
        if step:
            landed(block, az_sem, (step,))
        if step != 1:
            for turn, (part, late) in enumerate((("low", "high"), ("high", "low"))):
                for sems, which, peer, name in (
                    (ax_sem, 1, x_peer, part),
                    (ay_sem, 2, y_peer, late),
                ):
                    target = held.at[step, which, core]
                    push(cut(block, name), cut(target, name), sems, (step, turn), peer)
        push(block, block, ap_sem, (step, 0), twin)

    def cut(block, name):
        return block.at[:half] if name == "low" else block.at[half:]

    def relay(which, sems, index):
        push(held.at[0, which, core], held.at[1, which, core], sems, index, z_peers[1])

    def gather(which, sems, index):
        block = held.at[1, which, core]
        landed(block, sems, index)
        push(block, block, ap_sem, (1, which), twin)

    def forward(step):
        across_block = held.at[step, 3, core]
        block = held.at[step, 1, core]
        landed(block.at[:half], ax_sem, (step, 0))
        push(block.at[:half], across_block.at[:half], afy_sem, (step,), y_peer)
        block = held.at[step, 2, core]
        landed(block.at[half:], ay_sem, (step, 0))
        push(block.at[half:], across_block.at[half:], afx_sem, (step,), x_peer)

    def settle(step):
        block = held.at[step, 1, core]
        landed(block.at[half:], ax_sem, (step, 1))
        push(block, block, ap_sem, (step, 1), twin)
        block = held.at[step, 2, core]
        landed(block.at[:half], ay_sem, (step, 1))
        push(block, block, ap_sem, (step, 2), twin)
        if step == 0:
            relay(1, ax_sem, (1, 0))
            relay(2, ay_sem, (1, 0))

    def finish(step):
        block = held.at[step, 3, core]
        landed(block.at[:half], afy_sem, (step,))
        landed(block.at[half:], afx_sem, (step,))
        push(block, block, ap_sem, (step, 3), twin)
        if step == 0:
            relay(3, afx_sem, (1,))

    token_count = core_count * rows

    def share_planes():
        block = shares.at[0, 0, core]
        for step in (1, 2, 3):
            push(block, shares.at[step, 0, core], wz_sem, (step,), z_peers[step])

    def share_sides():
        for step in (1, 2, 3):
            landed(shares.at[step, 0, core], wz_sem, (step,))
        push(shares.at[:, 0, core], shares.at[:, 1, core], ws_sem, (0,), x_peer)
        push(shares.at[:, 0, core], shares.at[:, 2, core], ws_sem, (1,), y_peer)

    def share_across():
        landed(shares.at[:, 1, core], ws_sem, (0,))
        push(shares.at[:, 1, core], shares.at[:, 3, core], ws_sem, (2,), y_peer)

    def share_twin():
        landed(shares.at[:, 2, core], ws_sem, (1,))
        landed(shares.at[:, 3, core], ws_sem, (2,))
        push(shares.at[:, :, core], shares.at[:, :, core], ws_sem, (3,), twin)

    def share_column(step, which):
        share = shares[step, which, 0]
        for place in range(1, core_count):
            share = share + shares[step, which, place]
        expert = lax.broadcasted_iota(jnp.int32, share.shape, 0)
        row = jnp.sum(jnp.where(expert == shard, share, 0.0), axis=0, keepdims=True)
        column = jnp.transpose(jnp.broadcast_to(row, (token_count, token_count)))
        return jnp.concatenate([column] * (width // token_count), axis=1)

    def compute(step):
        for which in range(4):
            landed(held.at[step, which, other], ap_sem, (step, which))

        def one_part(turn, carry):
            which = jnp.where(turn == 0, 3, jnp.where(turn == 3, 0, turn))
            token_rows = held[step, which].reshape(token_count, width)
            gate_act = jnp.dot(token_rows, gate[...], preferred_element_type=wide)
            upper = jnp.dot(token_rows, up[...], preferred_element_type=wide)
            hidden = (gate_act / (1.0 + jnp.exp(-gate_act)) * upper).astype(kind)
            result = jnp.dot(hidden, down[...], preferred_element_type=wide)
            result = (result * share_column(step, which)).astype(kind)
            parts[step, which] = result.reshape(core_count, rows, width)
            part_copy(step, which).start()
            return carry

        lax.fori_loop(0, 4, one_part, 0)
        for which in range(4):
            sent.append(part_copy(step, which))

    def part_copy(step, which):
        return pushed(
            parts.at[step, which, other], twins.at[step, which], p_sem, (step, which), twin
        )

    def sums(step, which, begin, end):
        mine = parts[step, which, core, begin:end].astype(wide)
        return mine + twins[step, which, begin:end].astype(wide)

    def pair(step, which):
        landed(twins.at[step, which], p_sem, (step, which))
        return sums(step, which, 0, rows)

    def narrow(values):
        return values.astype(kind)

    def first(step):
        twins[step, 3] = narrow(pair(step, 3))
        push(twins.at[step, 3, :half], x_part.at[step], fx_sem, (step,), x_peer)
        push(twins.at[step, 3, half:], y_part.at[step], fy_sem, (step,), y_peer)

    def early(step):
        for which in (1, 2):
            landed(twins.at[step, which], p_sem, (step, which))
        twins[step, 1, :half] = narrow(sums(step, 1, 0, half))
        push(twins.at[step, 1, :half], x_all.at[step, :half], x_sem, (step, 0), x_peer)
        twins[step, 2, half:] = narrow(sums(step, 2, half, rows))
        push(twins.at[step, 2, half:], y_all.at[step, half:], y_sem, (step, 0), y_peer)

    def second(step):
        total = sums(step, 1, half, rows)
        landed(y_part.at[step], fy_sem, (step,))
        twins[step, 1, half:] = narrow(total + y_part[step].astype(wide))
        push(twins.at[step, 1, half:], x_all.at[step, half:], x_sem, (step, 1), x_peer)
        total = sums(step, 2, 0, half)
        landed(x_part.at[step], fx_sem, (step,))
        twins[step, 2, :half] = narrow(total + x_part[step].astype(wide))
        push(twins.at[step, 2, :half], y_all.at[step, :half], y_sem, (step, 1), y_peer)

    def third(step):
        total = pair(step, 0)
        for part in range(2):
            landed(x_all.at[step, part * half : (part + 1) * half], x_sem, (step, part))
            landed(y_all.at[step, (1 - part) * half : (2 - part) * half], y_sem, (step, part))
        total = total + x_all[step].astype(wide) + y_all[step].astype(wide)
        if step:
            twins[step, 0] = narrow(total)
            push(twins.at[step, 0], z_all.at[step], z_sem, (step,), z_peers[step])
        else:
            kept[...] = total

    seq_rows = keyed.shape[1]
    heads_here = lambdas.shape[1]
    value_size = gain.shape[1]
    pair_size = key_cols // heads_here
    key_half = seq_rows // 2

    def wider(values):
        return jnp.broadcast_to(values, (seq_rows, value_size))

    turn_rows = seq_rows // 8
    map_size = pair_size // 2
    lane = lax.broadcasted_iota(jnp.int32, (turn_rows, pair_size), 1)
    leading = lax.rem(lane, map_size) < map_size // 2

    def rotated(source, rows_at, head, cosine, sine):
        values = source[rows_at, head * pair_size : (head + 1) * pair_size].astype(wide)
        ahead = pltpu.roll(values, pair_size - map_size // 2, 1)
        behind = pltpu.roll(values, map_size // 2, 1)
        return values * cosine + jnp.where(leading, ahead, behind) * sine

    def rotate_keys():
        def one_chunk(chunk, carry):
            rows_at = pl.ds(pl.multiple_of(chunk * turn_rows, turn_rows), turn_rows)
            place = lax.broadcasted_iota(jnp.int32, (turn_rows, pair_size), 0)
            place = place + (shard * seq_rows + chunk * turn_rows)
            angles = place.astype(wide) * turns[...]
            cosine, sine = jnp.cos(angles), jnp.sin(angles)
            sine = jnp.where(leading, -sine, sine)
            cosines[rows_at, :] = cosine
            sines[rows_at, :] = sine
            for head in range(heads_here):
                keyed[0, rows_at, head * pair_size : (head + 1) * pair_size] = narrow(
                    rotated(raw_key, rows_at, head, cosine, sine)
                )
            return carry

        lax.fori_loop(0, 8, one_chunk, 0)

    def rotate_queries():
        def one_chunk(chunk, carry):
            rows_at = pl.ds(pl.multiple_of(chunk * turn_rows, turn_rows), turn_rows)
            cosine, sine = cosines[rows_at, :], sines[rows_at, :]
            for head in range(heads_here):
                values = rotated(raw_query, rows_at, head, cosine, sine) * map_size ** (-0.5)
                for half_at in range(2):
                    unit = 2 * head + half_at
                    own_map = (lane // map_size) == half_at
                    queries[rows_at, unit * pair_size : (unit + 1) * pair_size] = narrow(
                        jnp.where(own_map, values, 0.0)
                    )
            return carry

        lax.fori_loop(0, 8, one_chunk, 0)

    def attend(which, diagonal):
        for unit in range(2 * heads_here):
            head = unit // 2
            scores = lax.dot_general(
                queries[:, unit * pair_size : (unit + 1) * pair_size],
                keyed[which, :, head * pair_size : (head + 1) * pair_size],
                (((1,), (1,)), ((), ())),
                preferred_element_type=wide,
            )
            if diagonal:
                key_pos = lax.broadcasted_iota(jnp.int32, scores.shape, 1)
                query_pos = lax.broadcasted_iota(jnp.int32, scores.shape, 0)
                scores = jnp.where(key_pos <= query_pos, scores, far_below)
            top = wider(jnp.max(scores, axis=1, keepdims=True))
            if not diagonal:
                top = jnp.maximum(top, highest[unit])
            expo = jnp.exp(scores - jnp.concatenate([top] * (seq_rows // value_size), axis=1))
            total = wider(jnp.sum(expo, axis=1, keepdims=True))
            first_col = key_cols + head * value_size
            value = jnp.dot(
                narrow(expo),
                keyed[which, :, first_col : first_col + value_size],
                preferred_element_type=wide,
            )
            if not diagonal:
                shrink = jnp.exp(highest[unit] - top)
                total = total + totals[unit] * shrink
                value = value + weighted[unit] * shrink
            highest[unit] = top
            totals[unit] = total
            weighted[unit] = value

    def attend_across(which):
        across_shard = (shard, across_x, across_y, across)[which]

        @pl.when(across_shard < shard)
        def _():
            attend(which, False)

    def project():
        for head in range(heads_here):
            first_map = weighted[2 * head] / totals[2 * head]
            second_map = weighted[2 * head + 1] / totals[2 * head + 1]
            combined = first_map - lambdas[:, head : head + 1] * second_map
            cols = slice(head * value_size, (head + 1) * value_size)
            head_rows[:, cols] = narrow(norm_rows(combined, gain[...]))

        def one_plane(plane, carry):
            plane_rows = head_rows[pl.ds(plane * core_count * rows, core_count * rows), :]
            result = jnp.dot(plane_rows, mix_weight[...], preferred_element_type=wide)
            mix_parts[plane] = narrow(result).reshape(core_count, rows, width)
            return carry

        lax.fori_loop(0, planes, one_plane, 0)
        push(mix_parts.at[:, other], mix_twins, mp_sem, (0,), twin)

    level = column // core_count

    def mix_pair(step):
        plane = column_at(step) // core_count
        return plane, mix_parts[plane, core].astype(wide) + mix_twins[plane].astype(wide)

    def mix_send():
        landed(mix_twins, mp_sem, (0,))
        for step in range(1, planes):
            plane, total = mix_pair(step)
            mix_twins[plane] = narrow(total)
            push(mix_twins.at[plane], mix_all.at[step], mz_sem, (step,), z_peers[step])

    def mix_finish():
        total = mix_pair(0)[1]
        for step in range(1, planes):
            landed(mix_all.at[step], mz_sem, (step,))
            total = total + mix_all[step].astype(wide)
        mix_out[...] = narrow(total)

    share_planes()
    send_planes()
    spread(0)
    for load in loads[4:8]:
        load.wait()
    rotate_keys()
    send_keys()
    rotate_queries()
    attend(0, True)
    share_sides()
    forward(0)
    settle(0)
    share_across()
    landed(keyed.at[1], kv_sem, (0,))
    push(keyed.at[1, :key_half], keyed.at[3, :key_half], kv_sem, (2,), y_peer)
    landed(keyed.at[2], kv_sem, (1,))
    push(keyed.at[2, key_half:], keyed.at[3, key_half:], kv_sem, (3,), x_peer)
    finish(0)
    spread(2)
    attend_across(1)
    attend_across(2)
    share_twin()
    landed(keyed.at[3, :key_half], kv_sem, (2,))
    landed(keyed.at[3, key_half:], kv_sem, (3,))
    attend_across(3)
    for load in loads[8:]:
        load.wait()
    project()
    forward(2)
    mix_send()
    gather(1, ax_sem, (1, 0))
    settle(2)
    spread(3)
    finish(2)
    forward(3)
    landed(shares.at[:, :, other], ws_sem, (3,))
    compute(2)
    first(2)
    finish(3)
    spread(1)
    gather(2, ay_sem, (1, 0))
    early(2)
    settle(3)
    gather(3, afx_sem, (1,))
    second(2)
    compute(3)
    first(3)
    early(3)
    third(2)
    compute(1)
    first(1)
    second(3)
    compute(0)
    early(1)
    third(3)
    second(1)
    first(0)
    early(0)
    third(1)
    second(0)
    mix_finish()
    third(0)
    total = kept[...]
    for step in range(1, planes):
        landed(z_all.at[step], z_sem, (step,))
        total = total + z_all[step].astype(wide)
    out[...] = narrow(total)
    for copy in sent:
        copy.wait_send()


def run_layer(
    moe_input, moe_gain, expert_ids, route_weight, gate_weight, up_weight, down_weight,
    mix_query, mix_key, mix_value, turns, mix_weight, lambdas, gain, column_count,
):
    planes = column_count // core_count
    rows, width = moe_input.shape
    kind = moe_input.dtype
    arrays = [
        moe_input, moe_gain, expert_ids, route_weight, gate_weight, up_weight, down_weight,
        mix_query, mix_key, mix_value, turns, mix_weight, lambdas, gain,
    ]

    def room(*sizes):
        return pltpu.VMEM(sizes, kind)

    one = pltpu.SemaphoreType.DMA((2, planes))
    two = pltpu.SemaphoreType.DMA((2, planes, 2))
    four = pltpu.SemaphoreType.DMA((2, planes, 4))
    anywhere = pl.BlockSpec(memory_space=pl.ANY)
    near = pl.BlockSpec(memory_space=pltpu.VMEM)
    seq_rows, key_cols = mix_key.shape
    state = pltpu.VMEM((2 * lambdas.shape[1], seq_rows, gain.shape[1]), jnp.float32)

    def like(array):
        return pltpu.VMEM(array.shape, array.dtype)

    return pl.pallas_call(
        lambda *refs: layer_kernel(planes, *refs),
        out_shape=[pltpu.VMEM((rows, width), kind)] * 2,
        in_specs=[anywhere] * len(arrays),
        out_specs=[near, near],
        scratch_shapes=[
            like(moe_input),
            like(moe_gain),
            like(expert_ids),
            like(route_weight),
            like(mix_query),
            like(mix_key),
            like(turns),
            like(lambdas),
            like(gain),
            room(seq_rows, 2 * key_cols),
            pltpu.VMEM((seq_rows, turns.shape[1]), jnp.float32),
            pltpu.VMEM((seq_rows, turns.shape[1]), jnp.float32),
            room(4, seq_rows, key_cols + mix_value.shape[1]),
            room(*mix_weight.shape),
            state,
            state,
            state,
            room(seq_rows, mix_weight.shape[0]),
            room(planes, core_count, rows, width),
            room(planes, rows, width),
            room(planes, rows, width),
            room(planes, 4, core_count, rows, width),
            room(*gate_weight.shape),
            room(*up_weight.shape),
            room(*down_weight.shape),
            room(planes, 4, core_count, rows, width),
            room(planes, 4, rows, width),
            room(planes, rows // 2, width),
            room(planes, rows // 2, width),
            room(planes, rows, width),
            room(planes, rows, width),
            room(planes, rows, width),
            pltpu.VMEM((rows, width), jnp.float32),
            pltpu.VMEM((planes, 4, core_count, share_rows, core_count * rows), jnp.float32),
            one,
            one,
            pltpu.SemaphoreType.DMA((2, 4)),
            pltpu.SemaphoreType.DMA((2, 1)),
            one,
            pltpu.SemaphoreType.DMA((len(arrays),)),
            one, two, two, one, one, four, four, one, one, two, two, one,
        ],
        compiler_params=pltpu.CompilerParams(
            collective_id=0, has_side_effects=True, vmem_limit_bytes=62 * 1024 * 1024
        ),
        cost_estimate=pl.CostEstimate(flops=0, bytes_accessed=240000000, transcendentals=0),
        name="run_layer",
    )(*arrays)


def route_shares(expert_ids, route_weight, core):
    choices, rows = expert_ids.shape
    expert = lax.broadcasted_iota(jnp.int32, (share_rows, rows), 0)
    share = jnp.zeros(expert.shape, jnp.float32)
    for choice in range(choices):
        chosen = expert_ids[choice : choice + 1, :] == expert
        share = share + jnp.where(chosen, route_weight[choice : choice + 1, :], 0.0)
    empty = jnp.zeros_like(share)
    return jnp.concatenate(
        [jnp.where(core == place, share, empty) for place in range(core_count)], axis=1
    )


def experts_exchanged(
    moe_input, moe_gain, expert_ids, route_weight, gate_weight, up_weight, down_weight
):
    ep_size = lax.axis_size("ep")
    rows_b = moe_input.shape[0]
    top_count = expert_ids.shape[1]
    exp_here = gate_weight.shape[0]
    experts = exp_here * ep_size
    slot_count = 3 * rows_b * top_count // (2 * experts)
    normed = norm_rows(moe_input.astype(jnp.float32), moe_gain).astype(jnp.bfloat16)
    flat_ids = expert_ids.reshape(rows_b * top_count)
    member = (flat_ids[:, None] == jnp.arange(experts, dtype=jnp.int32)[None, :]).astype(jnp.int32)
    slot_rank = jnp.sum(member * (jnp.cumsum(member, axis=0) - 1), axis=1)
    target = (slot_rank * experts + flat_ids).reshape(rows_b, top_count)
    selector = (
        jnp.transpose(target)[:, :, None]
        == jnp.arange(slot_count * experts, dtype=jnp.int32)[None, None, :]
    ).astype(jnp.bfloat16)
    dispatched = jnp.einsum(
        "krs,rd->sd", selector, normed, preferred_element_type=jnp.float32
    ).astype(jnp.bfloat16)
    outgoing = dispatched.reshape(1, slot_count, experts, -1)
    arrived = lax.all_to_all(outgoing, "ep", split_axis=2, concat_axis=0, tiled=True)
    expert_rows = arrived.reshape(ep_size * slot_count, exp_here, -1)
    row_block = lax.all_gather(expert_rows, "tp", axis=0, tiled=True)
    gate_act = jnp.einsum(
        "mxd,xdf->mxf", row_block, gate_weight, preferred_element_type=jnp.float32
    )
    upper = jnp.einsum("mxd,xdf->mxf", row_block, up_weight, preferred_element_type=jnp.float32)
    hidden = (jax.nn.silu(gate_act) * upper).astype(jnp.bfloat16)
    row_block = hidden
    expert_sum = lax.psum_scatter(
        jnp.einsum(
            "mxf,xfd->mxd", row_block, down_weight, preferred_element_type=jnp.float32
        ).astype(jnp.bfloat16),
        "tp",
        scatter_dimension=0,
        tiled=True,
    )
    returning = expert_sum.reshape(ep_size, slot_count, exp_here, -1)
    returned = lax.all_to_all(returning, "ep", split_axis=0, concat_axis=2, tiled=True)
    results = returned.reshape(slot_count * experts, -1)
    chosen = jnp.einsum("krs,sd->krd", selector, results, preferred_element_type=jnp.float32)
    combined = jnp.sum(chosen * jnp.transpose(route_weight)[:, :, None], axis=0)
    return combined.astype(jnp.bfloat16)


def body(
    mix_query,
    mix_key,
    mix_value,
    head_lambda,
    head_gain,
    out_weight,
    moe_input,
    moe_gain,
    expert_ids,
    route_weight,
    gate_weight,
    up_weight,
    down_weight,
):
    seq_rows = mix_query.shape[0]
    heads_here = head_lambda.shape[0]
    head_size = mix_query.shape[1] // (2 * heads_here)
    value_size = mix_value.shape[1] // heads_here
    ep_size = lax.axis_size("ep")
    my_shard = lax.axis_index("ep")
    tp_size = lax.axis_size("tp")
    square = ep_size == 4 and tp_size == 4 * core_count
    if square and gate_weight.shape[0] == 1 and ep_size <= share_rows:
        frequency = rotary_base ** (-np.arange(head_size // 2) * 2.0 / head_size)
        moe_output, mix_output = run_layer(
            moe_input,
            moe_gain[None, :],
            jnp.transpose(expert_ids),
            jnp.transpose(route_weight),
            gate_weight[0],
            up_weight[0],
            down_weight[0],
            mix_query,
            mix_key,
            mix_value,
            jnp.asarray(np.tile(frequency, 4)[None, :], jnp.float32),
            out_weight,
            head_lambda[None, :],
            head_gain[None, :],
            tp_size,
        )
        return (mix_output, moe_output)
    query_pos = my_shard * seq_rows + jnp.arange(seq_rows, dtype=jnp.int32)
    queries = rotate(
        mix_query.astype(jnp.float32).reshape(seq_rows, heads_here, 2, head_size), query_pos
    )
    queries = (queries * head_size ** (-0.5)).astype(jnp.bfloat16)
    rotated_keys = rotate(
        mix_key.astype(jnp.float32).reshape(seq_rows, heads_here, 2, head_size), query_pos
    )
    rotated_keys = rotated_keys.astype(jnp.bfloat16).reshape(seq_rows, heads_here * 2 * head_size)
    stacked = jnp.concatenate([rotated_keys, mix_value], axis=1)
    query_last = jnp.max(query_pos)
    initial = (
        jnp.full((heads_here, 2, seq_rows), far_below, jnp.float32),
        jnp.zeros((heads_here, 2, seq_rows), jnp.float32),
        jnp.zeros((heads_here, 2, seq_rows, value_size), jnp.float32),
    )
    attention_state = fold_keys(
        initial, lax.all_gather(stacked, "ep", axis=0, tiled=True), queries, query_pos, query_last
    )
    running_max, totals, weighted = attention_state
    lambdas = head_lambda[:, None, None]
    combined_heads = (
        weighted[:, 0] / totals[:, 0][..., None]
        - lambdas * weighted[:, 1] / totals[:, 1][..., None]
    )
    combined_heads = norm_rows(combined_heads, head_gain).astype(jnp.bfloat16)
    head_rows = jnp.transpose(combined_heads, (1, 0, 2)).reshape(seq_rows, heads_here * value_size)
    mix_partial = jnp.dot(head_rows, out_weight, preferred_element_type=jnp.float32)
    mix_sum = lax.psum_scatter(
        mix_partial.astype(jnp.bfloat16), "tp", scatter_dimension=0, tiled=True
    )
    moe_args = (
        moe_input, moe_gain, expert_ids, route_weight, gate_weight, up_weight, down_weight
    )
    return (mix_sum, experts_exchanged(*moe_args))


def solution(mesh):
    return jax.shard_map(
        body,
        mesh=mesh,
        in_specs=(
            P("ep", "tp"),
            P("ep", "tp"),
            P("ep", "tp"),
            P("tp"),
            P(),
            P("tp", None),
            P(("ep", "tp"), None),
            P(),
            P(("ep", "tp"), None),
            P(("ep", "tp"), None),
            P("ep", None, "tp"),
            P("ep", None, "tp"),
            P("ep", "tp", None),
        ),
        out_specs=(P(("ep", "tp"), None), P(("ep", "tp"), None)),
        check_vma=False,
    )
```
